512 devices in a mesh: fs: 64 (over z, y), tp: 8 (over x, core).
Axes of the slice: x: 4, y: 8, z: 8, core: 2. Of those that a mesh axis runs over, the one named last changes fastest.
Arguments:
- later_input: bfloat16 [12288, 2048], P(('fs', 'tp')), may hold values from -6 to 6
- earlier_input: bfloat16 [12288, 2048], P(('fs', 'tp')), may hold values from -6 to 6
- cotangent: bfloat16 [12288, 2048], P(('fs', 'tp')), may hold values from -24 to 24
- gate_weight: bfloat16 [2048, 3072], P('fs', 'tp'), may hold values from -0.125 to 0.125
- up_weight: bfloat16 [2048, 3072], P('fs', 'tp'), may hold values from -0.125 to 0.125
- down_weight: bfloat16 [2048, 3072], P('fs', 'tp'), may hold values from -0.109375 to 0.109375
- down_grad_sum: float32 [2048, 3072], P('fs', 'tp'), may hold values from -6 to 6
Outputs:
- later_output: bfloat16 [12288, 2048], P(('fs', 'tp'))
- earlier_grad_input: bfloat16 [12288, 2048], P(('fs', 'tp'))
- new_down_grad_sum: float32 [2048, 3072], P('fs', 'tp')
The draws below stay inside these ranges and needn't reach their ends.
All inputs are finite; a program needn't handle non-finite values.
Results may differ from the reference program's by a relative error of at most 0.0057.
Values may be sent and summed in bfloat16 or wider, within the bound.
No kernel may reach another device: no remote copies, remote signals or barrier semaphores. Data moves between devices by JAX's collectives and lax.ppermute only.
A program may use at most 64 MiB of HBM per device.

```python
import jax
import jax.numpy as jnp
from jax import lax

D = 2048
FF = 3072
TOKENS = 12288
N_TP = 8


def raised(result, key, source, target, blocks, factor):
    owner, partner = [(jnp.arange(result.shape[axis_at]) // (result.shape[axis_at] // blocks)).reshape([-1 if axis == axis_at else 1 for axis in range(result.ndim)]) for axis_at in (source, target)]
    chosen = jax.random.permutation(key, blocks)[partner]
    strong = (owner == chosen) | (owner == (partner + blocks // 2) % blocks)
    return jnp.where(strong, factor * result, result)


def block_scale(rng, shape, split, low, top_value):
    factor_of, own = 1.0, jax.random.fold_in(rng, 6)
    for position, parts in split:
        heights = jnp.exp(jax.random.uniform(jax.random.fold_in(own, position), (parts,), jnp.float32, low / len(split), top_value / len(split)))
        factor_of = factor_of * jnp.repeat(heights, shape[position] // parts).reshape([-1 if axis == position else 1 for axis in range(len(shape))])
    return factor_of


def noise(stream_key, dims, deviation, most, shards=(), kind=jnp.bfloat16):
    loudness = block_scale(stream_key, dims, shards, -0.22, 0.18) if shards else 1.0
    entries = jax.random.normal(stream_key, dims, jnp.float32) * deviation * loudness
    return jnp.minimum(jnp.maximum(entries, -most), most).astype(kind)


def bell_draw_with(own_key, dims, deviation, most, split, heavy, held_as=jnp.bfloat16):
    entries = deviation * jax.random.normal(own_key, dims, jnp.float32)
    if split:
        entries = entries * block_scale(own_key, dims, split, -0.22, 0.18)
    return jnp.clip(raised(entries, jax.random.fold_in(own_key, 3), *heavy), -most, most).astype(held_as)


def setup_inputs(seed: int = 0) -> dict:
    keys = jax.random.split(jax.random.key(seed), 8)
    later_input = noise(keys[0], (TOKENS, D), 1.0, 6.0, ((0, 512),))
    earlier_input = noise(keys[1], (TOKENS, D), 1.0, 6.0, ((0, 512),))
    cotangent = bell_draw_with(keys[2], (TOKENS, D), 1.0, 24.0, ((0, 512),), (0, 1, 512, 6.0))
    gate_weight = noise(keys[3], (D, FF), D ** -0.5, 0.125, ((0, 64), (1, 8)))
    up_weight = noise(keys[4], (D, FF), D ** -0.5, 0.125, ((0, 64), (1, 8)))
    down_weight = noise(keys[5], (D, FF), FF ** -0.5, 0.109375, ((0, 64), (1, 8)))
    down_grad_sum = noise(keys[6], (D, FF), 1.0, 6.0, ((0, 64), (1, 8)), jnp.float32)
    return dict(later_input=later_input, earlier_input=earlier_input, cotangent=cotangent, gate_weight=gate_weight, up_weight=up_weight, down_weight=down_weight, down_grad_sum=down_grad_sum)


def partial_rows(gradients, weights, first_unit, last_unit):
    return jnp.dot(gradients[:, first_unit:last_unit], weights[:, first_unit:last_unit].T, preferred_element_type=jnp.float32)


def rounded_sum(total, partial_value):
    kept = lax.optimization_barrier(partial_value.astype(jnp.bfloat16))
    return total + kept.astype(jnp.float32)


def reference(later_input, earlier_input, cotangent, gate_weight, up_weight, down_weight, down_grad_sum):
    block_width = FF // N_TP
    gate_later = jnp.dot(later_input, gate_weight, preferred_element_type=jnp.float32)
    up_later = jnp.dot(later_input, up_weight, preferred_element_type=jnp.float32)
    hidden_later = (jax.nn.silu(gate_later) * up_later).astype(jnp.bfloat16)
    output_total = jnp.zeros((TOKENS, D), jnp.float32)
    for block_index in range(N_TP):
        first_unit = block_index * block_width
        partial_value = partial_rows(hidden_later, down_weight, first_unit, first_unit + block_width)
        output_total = rounded_sum(output_total, partial_value)
    later_output = output_total.astype(jnp.bfloat16)

    gate_early = jnp.dot(earlier_input, gate_weight, preferred_element_type=jnp.float32)
    up_early = jnp.dot(earlier_input, up_weight, preferred_element_type=jnp.float32)
    sigmoid_gate = jax.nn.sigmoid(gate_early)
    activated = gate_early * sigmoid_gate
    hidden_early = (activated * up_early).astype(jnp.bfloat16)
    grad_hidden = jnp.dot(cotangent, down_weight, preferred_element_type=jnp.float32)
    grad_gate = (grad_hidden * up_early * sigmoid_gate * (1.0 + gate_early * (1.0 - sigmoid_gate))).astype(jnp.bfloat16)
    grad_up = (grad_hidden * activated).astype(jnp.bfloat16)
    input_total = jnp.zeros((TOKENS, D), jnp.float32)
    for block_index in range(N_TP):
        first_unit = block_index * block_width
        last_unit = first_unit + block_width
        partial_value = partial_rows(grad_gate, gate_weight, first_unit, last_unit) + partial_rows(grad_up, up_weight, first_unit, last_unit)
        input_total = rounded_sum(input_total, partial_value)
    earlier_grad_input = input_total.astype(jnp.bfloat16)

    weight_grad = jnp.dot(cotangent.T, hidden_early, preferred_element_type=jnp.float32)
    new_down_grad_sum = down_grad_sum + weight_grad * (TOKENS ** -0.5)
    return (later_output, earlier_grad_input, new_down_grad_sum)
```

```python
import jax
import jax.numpy as jnp
from jax import lax
from jax.sharding import Mesh
from jax.sharding import PartitionSpec as P

AXES = ("z", "y", "x", "c")
BF, F32 = jnp.bfloat16, jnp.float32


def shift(value, axis, step):
    count = lax.axis_size(axis)
    return lax.ppermute(value, axis, [(i, (i + step) % count) for i in range(count)])


def spread(value, axis):
    count = lax.axis_size(axis)
    return lax.all_to_all(jnp.broadcast_to(value, (count, *value.shape)), axis, 0, 0)


def ring_gather(first, second, axis_first, axis_second):
    half = first.shape[0] // 2
    state = {
        (ring, sign): chunk
        for ring, chunk in ((0, first), (1, second))
        for sign in (1, -1)
    }
    axes = (axis_first, axis_second)
    yield 0, 0, None, first
    yield 1, 0, None, second
    for hop in range(1, 4):
        moved = {key: shift(chunk, axes[key[0]], key[1]) for key, chunk in state.items()}
        for (ring, sign), chunk in moved.items():
            yield ring, -sign * hop, None, chunk
        state = moved
    for (ring, sign), chunk in state.items():
        part = chunk[:half] if sign == 1 else chunk[half:]
        yield ring, 4, 0 if sign == 1 else 1, shift(part, axes[ring], sign)


def gather_weights(weights):
    rows, cols = weights.shape
    half = rows // 2
    nz, ny = lax.axis_size("z"), lax.axis_size("y")
    z, y = lax.axis_index("z"), lax.axis_index("y")
    top = spread(weights[:half], "y")
    bottom = spread(weights[half:], "z")
    whole = jnp.zeros((nz, ny, 2, half, cols), weights.dtype)
    for ring, offset, part, chunk in ring_gather(top, bottom, "z", "y"):
        lead = 0 if part is None else part * (chunk.shape[0])
        if ring == 0:
            at = ((z + offset) & (nz - 1), lead, 0, 0, 0)
            whole = lax.dynamic_update_slice(whole, chunk[None, :, None], at)
        else:
            at = (lead, (y + offset) & (ny - 1), 1, 0, 0)
            whole = lax.dynamic_update_slice(whole, chunk[:, None, None], at)
    return whole.reshape(nz * ny * rows, cols)


def sum_f32(parts):
    return jnp.sum(parts.astype(F32), axis=0)


def scatter_rows(full, rows):
    cols = full.shape[1]
    nz, ny = lax.axis_size("z"), lax.axis_size("y")
    parts = full.astype(BF).reshape(nz, ny, 2, rows // 2, cols)
    top = lax.all_to_all(jnp.moveaxis(parts[:, :, 0], 1, 0), "y", 0, 0)
    bottom = lax.all_to_all(parts[:, :, 1], "z", 0, 0)
    top = lax.all_to_all(sum_f32(top).astype(BF), "z", 0, 0)
    bottom = lax.all_to_all(sum_f32(bottom).astype(BF), "y", 0, 0)
    return jnp.concatenate([sum_f32(top), sum_f32(bottom)], axis=0)


def contract_last(leading, trailing):
    return lax.dot_general(
        leading, trailing, (((1,), (1,)), ((), ())), preferred_element_type=F32
    )


def give_rows(partial, rows):
    width = partial.shape[1]
    own, other = jnp.split(partial, 2, axis=0)
    both = (own + shift(other.astype(BF), "c", 1).astype(F32)).astype(BF)
    return sum_f32(lax.all_to_all(both.reshape(-1, rows, width), "x", 0, 0)).astype(BF)


def shards(later, early, cotangent, gate_w, up_w, down_w, down_grad_sum):
    rows, width = later.shape
    hidden = gate_w.shape[1]
    tokens = spread(jnp.concatenate([later, early, cotangent], axis=1), "x")
    tokens = tokens.reshape(-1, 3 * width)
    tokens = jnp.concatenate([tokens, shift(tokens, "c", 1)], axis=0)
    later_rows, early_rows, grad_rows = jnp.split(tokens, 3, axis=1)
    whole = gather_weights(jnp.concatenate([gate_w, up_w, down_w], axis=1))
    gate_whole, up_whole, down_whole = jnp.split(whole, 3, axis=1)

    gate_early = jnp.dot(early_rows, gate_whole, preferred_element_type=F32)
    up_early = jnp.dot(early_rows, up_whole, preferred_element_type=F32)
    sig = jax.nn.sigmoid(gate_early)
    activated = gate_early * sig
    hidden_early = (activated * up_early).astype(BF)
    down_grad = lax.dot_general(
        grad_rows, hidden_early, (((0,), (0,)), ((), ())), preferred_element_type=F32
    )
    summed = scatter_rows(down_grad, gate_w.shape[0])

    gate_later = jnp.dot(later_rows, gate_whole, preferred_element_type=F32)
    up_later = jnp.dot(later_rows, up_whole, preferred_element_type=F32)
    hidden_later = (jax.nn.silu(gate_later) * up_later).astype(BF)
    later_output = give_rows(contract_last(hidden_later, down_whole), rows)

    grad_hidden = jnp.dot(grad_rows, down_whole, preferred_element_type=F32)
    grad_gate = (grad_hidden * up_early * sig * (1.0 + gate_early * (1.0 - sig))).astype(BF)
    grad_up = (grad_hidden * activated).astype(BF)
    input_partial = contract_last(grad_gate, gate_whole) + contract_last(grad_up, up_whole)
    earlier_grad_input = give_rows(input_partial, rows)

    count = lax.axis_size("z") * lax.axis_size("y") * lax.axis_size("x") * lax.axis_size("c")
    factor = (rows * count) ** (-0.5)
    return later_output, earlier_grad_input, down_grad_sum + summed * factor


def solution(mesh):
    split = Mesh(mesh.devices.reshape(8, 8, 4, 2), AXES)
    tokens, weights = P(AXES, None), P(("z", "y"), ("x", "c"))
    return jax.shard_map(
        shards,
        mesh=split,
        in_specs=(tokens,) * 3 + (weights,) * 4,
        out_specs=(tokens, tokens, weights),
        check_vma=False,
    )
```

```python
import jax
import jax.numpy as jnp
from jax import lax
from jax.sharding import Mesh
from jax.sharding import PartitionSpec as P

AXES = ("z", "y", "x", "c")
FS = ("z", "y")
STEPS = (0, 1, -1, 2)
BF, F32 = jnp.bfloat16, jnp.float32


def shift(value, axis, step):
    count = lax.axis_size(axis)
    if step == 0:
        return value
    return lax.ppermute(value, axis, [(i, (i + step) % count) for i in range(count)])


def collect_tokens(own):
    line = jnp.concatenate([shift(own, "x", step) for step in STEPS], axis=0)
    return jnp.concatenate([line, shift(line, "c", 1)], axis=0)


def give_rows(partial, rows):
    own, other = jnp.split(partial, 2, axis=0)
    both = (own + shift(other.astype(BF), "c", 1).astype(F32)).astype(BF)
    total = jnp.zeros((rows, partial.shape[1]), F32)
    for at, step in enumerate(STEPS):
        total += shift(both[at * rows : (at + 1) * rows], "x", -step).astype(F32)
    return total.astype(BF)


def contract_last(leading, trailing):
    return lax.dot_general(
        leading, trailing, (((1,), (1,)), ((), ())), preferred_element_type=F32
    )


def shards(later, early, cotangent, gate_w, up_w, down_w, down_grad_sum):
    rows, width = later.shape
    weights = jnp.concatenate([gate_w, up_w, down_w], axis=1)
    whole = lax.all_gather(weights, FS, axis=0, tiled=True)
    gate_whole, up_whole, down_whole = jnp.split(whole, 3, axis=1)
    tokens = collect_tokens(jnp.concatenate([later, early, cotangent], axis=1))
    later_rows, early_rows, grad_rows = jnp.split(tokens, 3, axis=1)

    gate_early = jnp.dot(early_rows, gate_whole, preferred_element_type=F32)
    up_early = jnp.dot(early_rows, up_whole, preferred_element_type=F32)
    sig = jax.nn.sigmoid(gate_early)
    activated = gate_early * sig
    hidden_early = (activated * up_early).astype(BF)
    down_grad = lax.dot_general(
        grad_rows, hidden_early, (((0,), (0,)), ((), ())), preferred_element_type=F32
    ).astype(BF)
    later_rows, grad_rows, down_grad = lax.optimization_barrier(
        (later_rows, grad_rows, down_grad)
    )
    parts = down_grad.reshape(-1, *gate_w.shape)
    received = lax.all_to_all(parts, FS, 0, 0)

    grad_hidden = jnp.dot(grad_rows, down_whole, preferred_element_type=F32)
    grad_gate = (grad_hidden * up_early * sig * (1.0 + gate_early * (1.0 - sig))).astype(BF)
    grad_up = (grad_hidden * activated).astype(BF)
    input_partial = contract_last(grad_gate, gate_whole) + contract_last(grad_up, up_whole)
    earlier_grad_input = give_rows(input_partial, rows)

    gate_later = jnp.dot(later_rows, gate_whole, preferred_element_type=F32)
    up_later = jnp.dot(later_rows, up_whole, preferred_element_type=F32)
    hidden_later = (jax.nn.silu(gate_later) * up_later).astype(BF)
    later_output = give_rows(contract_last(hidden_later, down_whole), rows)

    summed = jnp.sum(received.astype(F32), axis=0)
    factor = (rows * lax.axis_size(AXES)) ** (-0.5)
    return later_output, earlier_grad_input, down_grad_sum + summed * factor


def solution(mesh):
    split = Mesh(mesh.devices.reshape(8, 8, 4, 2), AXES)
    tokens, weights = P(AXES, None), P(FS, ("x", "c"))
    return jax.shard_map(
        shards,
        mesh=split,
        in_specs=(tokens,) * 3 + (weights,) * 4,
        out_specs=(tokens, tokens, weights),
        check_vma=False,
    )
```

```python
import jax
import jax.numpy as jnp
from jax import lax
from jax.sharding import Mesh
from jax.sharding import PartitionSpec as P


AXES = ("z", "y", "x", "c")
FS = ("z", "y")
STEPS = (0, 1, -1, 2)
BF, F32 = jnp.bfloat16, jnp.float32


def shift(value, axis, step):
    count = lax.axis_size(axis)
    if step == 0:
        return value
    return lax.ppermute(value, axis, [(i, (i + step) % count) for i in range(count)])


def spread(value, axis):
    count = lax.axis_size(axis)
    return lax.all_to_all(jnp.broadcast_to(value, (count, *value.shape)), axis, 0, 0)


def after(value, *others):
    return lax.optimization_barrier((value, *others))[0]


def gather_down(down):
    line = spread(down, "z")
    count = lax.axis_size("y")
    half = line.shape[0] // 2
    mine = lax.axis_index("y")
    whole = jnp.zeros((line.shape[0], count, *down.shape), down.dtype)

    def put(whole, chunk, offset, lead):
        at = (lead, (mine + offset) & (count - 1), 0, 0)
        return lax.dynamic_update_slice(whole, chunk[:, None], at)

    whole = put(whole, line, 0, 0)
    ahead = behind = line
    for hop in range(1, count // 2):
        ahead, behind = shift(ahead, "y", 1), shift(behind, "y", -1)
        whole = put(put(whole, ahead, -hop, 0), behind, hop, 0)
    whole = put(whole, shift(ahead[:half], "y", 1), count // 2, 0)
    whole = put(whole, shift(behind[half:], "y", -1), count // 2, half)
    return whole.reshape(-1, down.shape[1])


def collect_tokens(own):
    line = jnp.concatenate([shift(own, "x", step) for step in STEPS], axis=0)
    return jnp.concatenate([line, shift(line, "c", 1)], axis=0)


def give_rows(partial, rows):
    own, other = jnp.split(partial, 2, axis=0)
    both = (own + shift(other.astype(BF), "c", 1).astype(F32)).astype(BF)
    total = jnp.zeros((rows, partial.shape[1]), F32)
    for at, step in enumerate(STEPS):
        total += shift(both[at * rows : (at + 1) * rows], "x", -step).astype(F32)
    return total.astype(BF)


def contract_last(leading, trailing):
    return lax.dot_general(
        leading, trailing, (((1,), (1,)), ((), ())), preferred_element_type=F32
    )


def shards(later, early, cotangent, gate_w, up_w, down_w, down_grad_sum):
    rows, _ = later.shape
    line = spread(jnp.concatenate([gate_w, up_w], axis=1), "y")
    line = line.reshape(-1, line.shape[-1])
    whole = lax.all_gather(line, "z", axis=0, tiled=True)
    gate_whole, up_whole = jnp.split(whole, 2, axis=1)
    tokens = collect_tokens(jnp.concatenate([later, early, cotangent], axis=1))
    later_rows, early_rows, grad_rows = jnp.split(tokens, 3, axis=1)
    down_whole = gather_down(after(down_w, line))

    gate_early = jnp.dot(early_rows, gate_whole, preferred_element_type=F32)
    up_early = jnp.dot(early_rows, up_whole, preferred_element_type=F32)
    sig = jax.nn.sigmoid(gate_early)
    activated = gate_early * sig
    hidden_early = (activated * up_early).astype(BF)
    down_grad = lax.dot_general(
        grad_rows, hidden_early, (((0,), (0,)), ((), ())), preferred_element_type=F32
    ).astype(BF)
    received = lax.all_to_all(down_grad.reshape(-1, *gate_w.shape), FS, 0, 0)

    grad_hidden = jnp.dot(grad_rows, down_whole, preferred_element_type=F32)
    grad_gate = grad_hidden * up_early * sig * (1.0 + gate_early * (1.0 - sig))
    grad_up = grad_hidden * activated
    input_partial = contract_last(grad_gate.astype(BF), gate_whole)
    input_partial += contract_last(grad_up.astype(BF), up_whole)

    gate_later = jnp.dot(later_rows, gate_whole, preferred_element_type=F32)
    up_later = jnp.dot(later_rows, up_whole, preferred_element_type=F32)
    hidden_later = (jax.nn.silu(gate_later) * up_later).astype(BF)
    output_partial = contract_last(hidden_later, down_whole)

    both = give_rows(jnp.concatenate([output_partial, input_partial], axis=1), rows)
    later_output, earlier_grad_input = jnp.split(both, 2, axis=1)

    summed = jnp.sum(received.astype(F32), axis=0)
    factor = (rows * lax.axis_size(AXES)) ** (-0.5)
    return later_output, earlier_grad_input, down_grad_sum + summed * factor


def solution(mesh):
    split = Mesh(mesh.devices.reshape(8, 8, 4, 2), AXES)
    tokens, weights = P(AXES, None), P(FS, ("x", "c"))
    return jax.shard_map(
        shards,
        mesh=split,
        in_specs=(tokens,) * 3 + (weights,) * 4,
        out_specs=(tokens, tokens, weights),
        check_vma=False,
    )
```

```python
import jax
import jax.numpy as jnp
from jax import lax
from jax.sharding import Mesh
from jax.sharding import PartitionSpec as P


AXES = ("z", "y", "x", "c")
FS = ("z", "y")
STEPS = (0, 1, -1, 2)
BF, F32 = jnp.bfloat16, jnp.float32


def shift(value, axis, step):
    count = lax.axis_size(axis)
    if step == 0:
        return value
    return lax.ppermute(value, axis, [(i, (i + step) % count) for i in range(count)])


def spread(value, axis):
    count = lax.axis_size(axis)
    return lax.all_to_all(jnp.broadcast_to(value, (count, *value.shape)), axis, 0, 0)


def line_of(value, axis):
    count = lax.axis_size(axis)
    mine = lax.axis_index(axis)
    whole = jnp.zeros((count, *value.shape), value.dtype)
    for step in range(count):
        at = ((mine + step) & (count - 1), 0, 0)
        whole = lax.dynamic_update_slice(whole, shift(value, axis, -step)[None], at)
    return whole


def ring_gather(line):
    count = lax.axis_size("y")
    half = line.shape[0] // 2
    mine = lax.axis_index("y")
    whole = jnp.zeros((line.shape[0], count, *line.shape[1:]), line.dtype)

    def put(whole, chunk, offset, lead):
        at = (lead, (mine + offset) & (count - 1), 0, 0)
        return lax.dynamic_update_slice(whole, chunk[:, None], at)

    whole = put(whole, line, 0, 0)
    ahead = behind = line
    for hop in range(1, count // 2):
        ahead, behind = shift(ahead, "y", 1), shift(behind, "y", -1)
        whole = put(put(whole, ahead, -hop, 0), behind, hop, 0)
    whole = put(whole, shift(ahead[:half], "y", 1), count // 2, 0)
    whole = put(whole, shift(behind[half:], "y", -1), count // 2, half)
    return whole.reshape(-1, line.shape[-1])


def collect_tokens(own):
    line = jnp.concatenate([shift(own, "x", step) for step in STEPS], axis=0)
    return jnp.concatenate([line, shift(line, "c", 1)], axis=0)


def give_rows(partial, rows):
    own, other = jnp.split(partial, 2, axis=0)
    both = (own + shift(other.astype(BF), "c", 1).astype(F32)).astype(BF)
    total = jnp.zeros((rows, partial.shape[1]), F32)
    for at, step in enumerate(STEPS):
        total += shift(both[at * rows : (at + 1) * rows], "x", -step).astype(F32)
    return total.astype(BF)


def contract_last(leading, trailing):
    return lax.dot_general(
        leading, trailing, (((1,), (1,)), ((), ())), preferred_element_type=F32
    )


def shards(later, early, cotangent, gate_w, up_w, down_w, down_grad_sum):
    rows, _ = later.shape
    line = spread(jnp.concatenate([gate_w, up_w], axis=1), "y")
    line = line.reshape(-1, line.shape[-1])
    whole = lax.all_gather(line, "z", axis=0, tiled=True)
    gate_whole, up_whole = jnp.split(whole, 2, axis=1)
    down_line = line_of(down_w, "z")
    down_whole = ring_gather(down_line)
    tokens = jnp.concatenate([later, early, cotangent], axis=1)
    tokens = collect_tokens(tokens)
    later_rows, early_rows, grad_rows = jnp.split(tokens, 3, axis=1)

    gate_early = jnp.dot(early_rows, gate_whole, preferred_element_type=F32)
    up_early = jnp.dot(early_rows, up_whole, preferred_element_type=F32)
    sig = jax.nn.sigmoid(gate_early)
    activated = gate_early * sig
    hidden_early = (activated * up_early).astype(BF)
    down_grad = lax.dot_general(
        grad_rows, hidden_early, (((0,), (0,)), ((), ())), preferred_element_type=F32
    ).astype(BF)
    received = lax.all_to_all(down_grad.reshape(-1, *gate_w.shape), FS, 0, 0)

    grad_hidden = jnp.dot(grad_rows, down_whole, preferred_element_type=F32)
    grad_gate = grad_hidden * up_early * sig * (1.0 + gate_early * (1.0 - sig))
    grad_up = grad_hidden * activated
    input_partial = contract_last(grad_gate.astype(BF), gate_whole)
    input_partial += contract_last(grad_up.astype(BF), up_whole)

    gate_later = jnp.dot(later_rows, gate_whole, preferred_element_type=F32)
    up_later = jnp.dot(later_rows, up_whole, preferred_element_type=F32)
    hidden_later = (jax.nn.silu(gate_later) * up_later).astype(BF)
    output_partial = contract_last(hidden_later, down_whole)

    both = give_rows(jnp.concatenate([output_partial, input_partial], axis=1), rows)
    later_output, earlier_grad_input = jnp.split(both, 2, axis=1)

    summed = jnp.sum(received.astype(F32), axis=0)
    factor = (rows * lax.axis_size(AXES)) ** (-0.5)
    return later_output, earlier_grad_input, down_grad_sum + summed * factor


def solution(mesh):
    split = Mesh(mesh.devices.reshape(8, 8, 4, 2), AXES)
    tokens, weights = P(AXES, None), P(FS, ("x", "c"))
    return jax.shard_map(
        shards,
        mesh=split,
        in_specs=(tokens,) * 3 + (weights,) * 4,
        out_specs=(tokens, tokens, weights),
        check_vma=False,
    )
```

```python
import jax
import jax.numpy as jnp
from jax import lax
from jax.sharding import Mesh
from jax.sharding import PartitionSpec as P


AXES = ("z", "y", "x", "c")
FS = ("z", "y")
STEPS = (0, 1, -1, 2)
BF, F32 = jnp.bfloat16, jnp.float32


def shift(value, axis, step):
    count = lax.axis_size(axis)
    if step == 0:
        return value
    return lax.ppermute(value, axis, [(i, (i + step) % count) for i in range(count)])


def spread(value, axis):
    count = lax.axis_size(axis)
    return lax.all_to_all(jnp.broadcast_to(value, (count, *value.shape)), axis, 0, 0)


def ring_gather(line, axis):
    count = lax.axis_size(axis)
    half = line.shape[0] // 2
    mine = lax.axis_index(axis)
    at_dim = FS.index(axis)
    shape = list(line.shape)
    shape.insert(at_dim, count)
    whole = jnp.zeros(shape, line.dtype)

    def put(whole, chunk, offset, lead):
        at = [lead, 0, 0]
        at.insert(at_dim, (mine + offset) & (count - 1))
        return lax.dynamic_update_slice(whole, jnp.expand_dims(chunk, at_dim), at)

    whole = put(whole, line, 0, 0)
    ahead = behind = line
    for hop in range(1, count // 2):
        ahead, behind = shift(ahead, axis, 1), shift(behind, axis, -1)
        whole = put(put(whole, ahead, -hop, 0), behind, hop, 0)
    whole = put(whole, shift(ahead[:half], axis, 1), count // 2, 0)
    whole = put(whole, shift(behind[half:], axis, -1), count // 2, half)
    return whole.reshape(-1, line.shape[-1])


def collect_tokens(own):
    line = jnp.concatenate([shift(own, "x", step) for step in STEPS], axis=0)
    other = shift(line, "c", 1)
    return jnp.concatenate([line, other], axis=0)


def give_rows(partial, rows):
    own, other = jnp.split(partial, 2, axis=0)
    both = (own + shift(other.astype(BF), "c", 1).astype(F32)).astype(BF)
    total = jnp.zeros((rows, partial.shape[1]), F32)
    for at, step in enumerate(STEPS):
        total += shift(both[at * rows : (at + 1) * rows], "x", -step).astype(F32)
    return total.astype(BF)


def contract_last(leading, trailing):
    return lax.dot_general(
        leading, trailing, (((1,), (1,)), ((), ())), preferred_element_type=F32
    )


def shards(later, early, cotangent, gate_w, up_w, down_w, down_grad_sum):
    rows, _ = later.shape
    down_whole = lax.all_gather(down_w, FS, axis=0, tiled=True)
    gate_line = spread(gate_w, "y")
    up_line = spread(up_w, "z")
    tokens = jnp.concatenate([later, early, cotangent], axis=1)
    tokens = collect_tokens(tokens)
    gate_whole = ring_gather(gate_line, "z")
    up_whole = ring_gather(up_line, "y")
    later_rows, early_rows, grad_rows = jnp.split(tokens, 3, axis=1)

    gate_early = jnp.dot(early_rows, gate_whole, preferred_element_type=F32)
    up_early = jnp.dot(early_rows, up_whole, preferred_element_type=F32)
    sig = jax.nn.sigmoid(gate_early)
    activated = gate_early * sig
    hidden_early = (activated * up_early).astype(BF)
    down_grad = lax.dot_general(
        grad_rows, hidden_early, (((0,), (0,)), ((), ())), preferred_element_type=F32
    ).astype(BF)
    received = lax.all_to_all(down_grad.reshape(-1, *gate_w.shape), FS, 0, 0)

    grad_hidden = jnp.dot(grad_rows, down_whole, preferred_element_type=F32)
    grad_gate = grad_hidden * up_early * sig * (1.0 + gate_early * (1.0 - sig))
    grad_up = grad_hidden * activated
    input_partial = contract_last(grad_gate.astype(BF), gate_whole)
    input_partial += contract_last(grad_up.astype(BF), up_whole)

    gate_later = jnp.dot(later_rows, gate_whole, preferred_element_type=F32)
    up_later = jnp.dot(later_rows, up_whole, preferred_element_type=F32)
    hidden_later = (jax.nn.silu(gate_later) * up_later).astype(BF)
    output_partial = contract_last(hidden_later, down_whole)

    both = give_rows(jnp.concatenate([output_partial, input_partial], axis=1), rows)
    later_output, earlier_grad_input = jnp.split(both, 2, axis=1)

    summed = jnp.sum(received.astype(F32), axis=0)
    factor = (rows * lax.axis_size(AXES)) ** (-0.5)
    return later_output, earlier_grad_input, down_grad_sum + summed * factor


def solution(mesh):
    split = Mesh(mesh.devices.reshape(8, 8, 4, 2), AXES)
    tokens, weights = P(AXES, None), P(FS, ("x", "c"))
    return jax.shard_map(
        shards,
        mesh=split,
        in_specs=(tokens,) * 3 + (weights,) * 4,
        out_specs=(tokens, tokens, weights),
        check_vma=False,
    )
```

```python
import jax
import jax.numpy as jnp
from jax import lax
from jax.sharding import Mesh
from jax.sharding import PartitionSpec as P


AXES = ("z", "y", "x", "c")
FS = ("z", "y")
STEPS = (0, 1, -1, 2)
BF, F32 = jnp.bfloat16, jnp.float32


def shift(value, axis, step):
    count = lax.axis_size(axis)
    if step == 0:
        return value
    return lax.ppermute(value, axis, [(i, (i + step) % count) for i in range(count)])


def spread(value, axis):
    count = lax.axis_size(axis)
    return lax.all_to_all(jnp.broadcast_to(value, (count, *value.shape)), axis, 0, 0)


def gather_down(down):
    line = spread(down, "z")
    count = lax.axis_size("y")
    half = line.shape[0] // 2
    mine = lax.axis_index("y")
    whole = jnp.zeros((line.shape[0], count, *down.shape), down.dtype)

    def put(whole, chunk, offset, lead):
        at = (lead, (mine + offset) & (count - 1), 0, 0)
        return lax.dynamic_update_slice(whole, chunk[:, None], at)

    whole = put(whole, line, 0, 0)
    ahead = behind = line
    for hop in range(1, count // 2):
        ahead, behind = shift(ahead, "y", 1), shift(behind, "y", -1)
        whole = put(put(whole, ahead, -hop, 0), behind, hop, 0)
    whole = put(whole, shift(ahead[:half], "y", 1), count // 2, 0)
    whole = put(whole, shift(behind[half:], "y", -1), count // 2, half)
    return whole.reshape(-1, down.shape[1])


def collect_tokens(own):
    line = jnp.concatenate([shift(own, "x", step) for step in STEPS], axis=0)
    other = shift(line, "c", 1)
    return jnp.concatenate([line, other], axis=0)


def give_rows(partial, rows):
    own, other = jnp.split(partial, 2, axis=0)
    both = (own + shift(other.astype(BF), "c", 1).astype(F32)).astype(BF)
    total = jnp.zeros((rows, partial.shape[1]), F32)
    for at, step in enumerate(STEPS):
        total += shift(both[at * rows : (at + 1) * rows], "x", -step).astype(F32)
    return total.astype(BF)


def contract_last(leading, trailing):
    return lax.dot_general(
        leading, trailing, (((1,), (1,)), ((), ())), preferred_element_type=F32
    )


def shards(later, early, cotangent, gate_w, up_w, down_w, down_grad_sum):
    rows, _ = later.shape
    line = spread(jnp.concatenate([gate_w, up_w], axis=1), "y")
    line = line.reshape(-1, line.shape[-1])
    whole = lax.all_gather(line, "z", axis=0, tiled=True)
    gate_whole, up_whole = jnp.split(whole, 2, axis=1)
    tokens = jnp.concatenate([later, early, cotangent], axis=1)
    tokens = collect_tokens(tokens)
    later_rows, early_rows, grad_rows = jnp.split(tokens, 3, axis=1)
    down_whole = gather_down(down_w)

    gate_early = jnp.dot(early_rows, gate_whole, preferred_element_type=F32)
    up_early = jnp.dot(early_rows, up_whole, preferred_element_type=F32)
    sig = jax.nn.sigmoid(gate_early)
    activated = gate_early * sig
    hidden_early = (activated * up_early).astype(BF)
    down_grad = lax.dot_general(
        grad_rows, hidden_early, (((0,), (0,)), ((), ())), preferred_element_type=F32
    ).astype(BF)
    received = lax.all_to_all(down_grad.reshape(-1, *gate_w.shape), FS, 0, 0)

    grad_hidden = jnp.dot(grad_rows, down_whole, preferred_element_type=F32)
    grad_gate = grad_hidden * up_early * sig * (1.0 + gate_early * (1.0 - sig))
    grad_up = grad_hidden * activated
    input_partial = contract_last(grad_gate.astype(BF), gate_whole)
    input_partial += contract_last(grad_up.astype(BF), up_whole)

    gate_later = jnp.dot(later_rows, gate_whole, preferred_element_type=F32)
    up_later = jnp.dot(later_rows, up_whole, preferred_element_type=F32)
    hidden_later = (jax.nn.silu(gate_later) * up_later).astype(BF)
    output_partial = contract_last(hidden_later, down_whole)

    both = give_rows(jnp.concatenate([output_partial, input_partial], axis=1), rows)
    later_output, earlier_grad_input = jnp.split(both, 2, axis=1)

    summed = jnp.sum(received.astype(F32), axis=0)
    factor = (rows * lax.axis_size(AXES)) ** (-0.5)
    return later_output, earlier_grad_input, down_grad_sum + summed * factor


def solution(mesh):
    split = Mesh(mesh.devices.reshape(8, 8, 4, 2), AXES)
    tokens, weights = P(AXES, None), P(FS, ("x", "c"))
    return jax.shard_map(
        shards,
        mesh=split,
        in_specs=(tokens,) * 3 + (weights,) * 4,
        out_specs=(tokens, tokens, weights),
        check_vma=False,
    )
```

```python
import jax
import jax.numpy as jnp
from jax import lax
from jax.experimental import pallas as pl
from jax.experimental.pallas import tpu as pltpu
from jax.sharding import Mesh
from jax.sharding import PartitionSpec as P


AXES = ("z", "y", "x", "c")
FS = ("z", "y")
STEPS = (0, 1, -1, 2)
BLOCKS = 4
OFFSETS = (0, -1, 1, -2, 2, -3, 3, 4)
BF, F32 = jnp.bfloat16, jnp.float32


def shift(value, axis, step):
    count = lax.axis_size(axis)
    if step == 0:
        return value
    return lax.ppermute(value, axis, [(i, (i + step) % count) for i in range(count)])


def spread(value, axis):
    count = lax.axis_size(axis)
    return lax.all_to_all(jnp.broadcast_to(value, (count, *value.shape)), axis, 0, 0)


def gather_down(down):
    line = spread(down, "z")
    chunks, ahead, behind = [line], line, line
    for _ in range(3):
        ahead, behind = shift(ahead, "y", 1), shift(behind, "y", -1)
        chunks += [ahead, behind]
    return [*chunks, shift(ahead, "y", 1)]


def collect_tokens(own):
    pieces = [shift(own, "x", step) for step in STEPS]
    line = jnp.concatenate(pieces, axis=0)
    other = shift(line, "c", 1)
    return jnp.concatenate([line, other], axis=0)


def give_rows(own, other, rows):
    both = (own + shift(other, "c", 1).astype(F32)).astype(BF)
    total = 0.0
    for at, step in enumerate(STEPS):
        total += shift(both[:, at * rows : (at + 1) * rows], "x", -step).astype(F32)
    return total.astype(BF)


def dot_nt(leading, trailing):
    return lax.dot_general(
        leading, trailing, (((1,), (1,)), ((), ())), preferred_element_type=F32
    )


def early_kernel(token_ref, weight_ref, cot_ref, gate_ref, up_ref, grad_ref, sum_ref, hidden_ref):
    step = pl.program_id(0)
    half = gate_ref.shape[1]

    @pl.when(step == 0)
    def _():
        sum_ref[...] = jnp.zeros_like(sum_ref)

    @pl.when(step < BLOCKS)
    def _():
        sum_ref[...] += jnp.dot(token_ref[...], weight_ref[...], preferred_element_type=F32)

    @pl.when(step == BLOCKS - 1)
    def _():
        gate, up = sum_ref[:, :half], sum_ref[:, half:]
        gate_ref[...] = gate
        up_ref[...] = up
        hidden_ref[...] = (gate / (1.0 + jnp.exp(-gate)) * up).astype(BF)

    @pl.when(step >= BLOCKS)
    def _():
        grad_ref[...] = lax.dot_general(
            cot_ref[...], hidden_ref[...], (((0,), (0,)), ((), ())), preferred_element_type=F32
        ).astype(BF)


def early_part(tokens, whole):
    rows, width = tokens.shape[0], whole.shape[0]
    both, block = whole.shape[1], width // BLOCKS
    half = both // 2
    first = lambda k: jnp.minimum(k, BLOCKS - 1)
    then = lambda k: jnp.maximum(k - BLOCKS, 0)
    return pl.pallas_call(
        early_kernel,
        grid=(2 * BLOCKS,),
        in_specs=[
            pl.BlockSpec((rows, block), lambda k: (0, BLOCKS + first(k))),
            pl.BlockSpec((block, both), lambda k: (first(k), 0)),
            pl.BlockSpec((rows, block), lambda k: (0, 2 * BLOCKS + then(k))),
        ],
        out_specs=[
            pl.BlockSpec((rows, half), lambda k: (0, 0)),
            pl.BlockSpec((rows, half), lambda k: (0, 0)),
            pl.BlockSpec((block, half), lambda k: (then(k), 0)),
        ],
        out_shape=[
            jax.ShapeDtypeStruct((rows, half), F32),
            jax.ShapeDtypeStruct((rows, half), F32),
            jax.ShapeDtypeStruct((width, half), BF),
        ],
        scratch_shapes=[pltpu.VMEM((rows, both), F32), pltpu.VMEM((rows, half), BF)],
        compiler_params=pltpu.CompilerParams(
            dimension_semantics=("arbitrary",), vmem_limit_bytes=12 << 20
        ),
        cost_estimate=pl.CostEstimate(
            flops=6 * rows * width * half, transcendentals=rows * half, bytes_accessed=8 << 20
        ),
    )(tokens, whole, tokens)


def rest_kernel(
    row_ref, later_ref, cot_ref, weight_ref, gate_ref, up_ref, *others
):
    chunk_refs, (own_ref, other_ref) = others[:8], others[8:10]
    down_ref, sum_ref, grad_ref, hidden_ref, to_gate_ref, to_up_ref = others[10:]
    step = pl.program_id(0)
    half, lines = gate_ref.shape[1], down_ref.shape[0] // BLOCKS
    mine = own_ref.shape[1]

    @pl.when(step == 0)
    def _():
        sum_ref[...] = jnp.zeros_like(sum_ref)
        grad_ref[...] = jnp.zeros_like(grad_ref)
        for offset, chunk_ref in zip(OFFSETS, chunk_refs):
            at = (row_ref[0] + offset) & (len(OFFSETS) - 1)
            down_ref[:, pl.ds(at, 1)] = chunk_ref[...][:, None]

    @pl.when(step < BLOCKS)
    def _():
        down = down_ref[pl.ds(step * lines, lines)].reshape(-1, half)
        sum_ref[...] += jnp.dot(later_ref[...], weight_ref[...], preferred_element_type=F32)
        grad_ref[...] += jnp.dot(cot_ref[...], down, preferred_element_type=F32)

    @pl.when(step == BLOCKS - 1)
    def _():
        gate, up = sum_ref[:, :half], sum_ref[:, half:]
        hidden_ref[...] = (gate / (1.0 + jnp.exp(-gate)) * up).astype(BF)
        gate, grad = gate_ref[...], grad_ref[...]
        sig = 1.0 / (1.0 + jnp.exp(-gate))
        to_gate_ref[...] = (grad * up_ref[...] * sig * (1.0 + gate * (1.0 - sig))).astype(BF)
        to_up_ref[...] = (grad * (gate * sig)).astype(BF)

    @pl.when(step >= BLOCKS)
    def _():
        down = down_ref[pl.ds((step - BLOCKS) * lines, lines)].reshape(-1, half)
        out = dot_nt(hidden_ref[...], down)
        back = dot_nt(to_gate_ref[...], weight_ref[:, :half])
        back += dot_nt(to_up_ref[...], weight_ref[:, half:])
        own_ref[0], own_ref[1] = out[:mine], back[:mine]
        other_ref[0], other_ref[1] = out[mine:].astype(BF), back[mine:].astype(BF)


def rest_part(tokens, whole, gate_early, up_early, chunks):
    rows, (width, both) = tokens.shape[0], whole.shape
    block, half = width // BLOCKS, both // 2
    lines = chunks[0].shape[0]
    first = lambda k: jnp.minimum(k, BLOCKS - 1)
    then = lambda k: jnp.maximum(k - BLOCKS, 0)
    whole_of = lambda array: pl.BlockSpec(array.shape, lambda k: (0,) * array.ndim)
    out_block = pl.BlockSpec((2, rows // 2, block), lambda k: (0, 0, then(k)))
    return pl.pallas_call(
        rest_kernel,
        grid=(2 * BLOCKS,),
        in_specs=[
            pl.BlockSpec(memory_space=pltpu.SMEM),
            pl.BlockSpec((rows, block), lambda k: (0, first(k))),
            pl.BlockSpec((rows, block), lambda k: (0, 2 * BLOCKS + first(k))),
            pl.BlockSpec((block, both), lambda k: (k % BLOCKS, 0)),
            whole_of(gate_early),
            whole_of(up_early),
            *map(whole_of, chunks),
        ],
        out_specs=[out_block, out_block],
        out_shape=[
            jax.ShapeDtypeStruct((2, rows // 2, width), F32),
            jax.ShapeDtypeStruct((2, rows // 2, width), BF),
        ],
        scratch_shapes=[
            pltpu.VMEM((lines, len(chunks), *chunks[0].shape[1:]), BF),
            pltpu.VMEM((rows, both), F32),
            pltpu.VMEM((rows, half), F32),
            pltpu.VMEM((rows, half), BF),
            pltpu.VMEM((rows, half), BF),
            pltpu.VMEM((rows, half), BF),
        ],
        compiler_params=pltpu.CompilerParams(
            dimension_semantics=("arbitrary",), vmem_limit_bytes=16 << 20
        ),
        cost_estimate=pl.CostEstimate(
            flops=12 * rows * width * half, transcendentals=2 * rows * half, bytes_accessed=16 << 20
        ),
    )(
        lax.axis_index("y").astype(jnp.int32)[None],
        tokens,
        tokens,
        whole,
        gate_early,
        up_early,
        *chunks,
    )


def shards(later, early, cotangent, gate_w, up_w, down_w, down_grad_sum):
    rows, _ = later.shape
    line = spread(jnp.concatenate([gate_w, up_w], axis=1), "y")
    line = line.reshape(-1, line.shape[-1])
    whole = lax.all_gather(line, "z", axis=0, tiled=True)
    tokens = jnp.concatenate([later, early, cotangent], axis=1)
    tokens = collect_tokens(tokens)
    chunks = gather_down(down_w)

    gate_early, up_early, down_grad = early_part(tokens, whole)
    received = lax.all_to_all(down_grad.reshape(-1, *gate_w.shape), FS, 0, 0)

    own, other = rest_part(tokens, whole, gate_early, up_early, chunks)
    later_output, earlier_grad_input = give_rows(own, other, rows)

    summed = jnp.sum(received.astype(F32), axis=0)
    factor = (rows * lax.axis_size(AXES)) ** (-0.5)
    return later_output, earlier_grad_input, down_grad_sum + summed * factor


def solution(mesh):
    split = Mesh(mesh.devices.reshape(8, 8, 4, 2), AXES)
    tokens, weights = P(AXES, None), P(FS, ("x", "c"))
    return jax.shard_map(
        shards,
        mesh=split,
        in_specs=(tokens,) * 3 + (weights,) * 4,
        out_specs=(tokens, tokens, weights),
        check_vma=False,
    )
```

```python
import jax
import jax.numpy as jnp
from jax import lax
from jax.experimental import pallas as pl
from jax.experimental.pallas import tpu as pltpu
from jax.sharding import Mesh
from jax.sharding import PartitionSpec as P


AXES = ("z", "y", "x", "c")
FS = ("z", "y")
STEPS = (0, 1, -1, 2)
BLOCKS = 4
OFFSETS = (0, -1, 1, -2, 2, -3, 3, 4)
BF, F32 = jnp.bfloat16, jnp.float32


def shift(value, axis, step):
    count = lax.axis_size(axis)
    if step == 0:
        return value
    return lax.ppermute(value, axis, [(i, (i + step) % count) for i in range(count)])


def spread(value, axis):
    count = lax.axis_size(axis)
    return lax.all_to_all(jnp.broadcast_to(value, (count, *value.shape)), axis, 0, 0)


def gather_down(down):
    line = spread(down, "z")
    chunks, ahead, behind = [line], line, line
    for _ in range(1, 4):
        ahead, behind = shift(ahead, "y", 1), shift(behind, "y", -1)
        chunks += [ahead, behind]
    return [*chunks, shift(ahead, "y", 1)]


def collect_tokens(own):
    pieces = [shift(own, "x", step) for step in STEPS]
    line = jnp.concatenate(pieces, axis=0)
    other = shift(line, "c", 1)
    return jnp.concatenate([line, other], axis=0)


def give_rows(own, other, rows):
    both = (own + shift(other, "c", 1).astype(F32)).astype(BF)
    total = 0.0
    for at, step in enumerate(STEPS):
        total += shift(both[:, at * rows : (at + 1) * rows], "x", -step).astype(F32)
    return total.astype(BF)


def dot_nt(leading, trailing):
    return lax.dot_general(
        leading, trailing, (((1,), (1,)), ((), ())), preferred_element_type=F32
    )


def early_kernel(token_ref, weight_ref, cot_ref, gate_ref, up_ref, grad_ref, sum_ref, hidden_ref):
    step = pl.program_id(0)
    half = gate_ref.shape[1]

    @pl.when(step == 0)
    def _():
        sum_ref[...] = jnp.zeros_like(sum_ref)

    @pl.when(step < BLOCKS)
    def _():
        sum_ref[...] += jnp.dot(token_ref[...], weight_ref[...], preferred_element_type=F32)

    @pl.when(step == BLOCKS - 1)
    def _():
        gate, up = sum_ref[:, :half], sum_ref[:, half:]
        gate_ref[...] = gate
        up_ref[...] = up
        hidden_ref[...] = (gate / (1.0 + jnp.exp(-gate)) * up).astype(BF)

    @pl.when(step >= BLOCKS)
    def _():
        grad_ref[...] = lax.dot_general(
            cot_ref[...], hidden_ref[...], (((0,), (0,)), ((), ())), preferred_element_type=F32
        ).astype(BF)


def early_part(tokens, whole):
    rows, width = tokens.shape[0], whole.shape[0]
    both, block = whole.shape[1], width // BLOCKS
    half = both // 2
    first = lambda k: jnp.minimum(k, BLOCKS - 1)
    then = lambda k: jnp.maximum(k - BLOCKS, 0)
    return pl.pallas_call(
        early_kernel,
        grid=(2 * BLOCKS,),
        in_specs=[
            pl.BlockSpec((rows, block), lambda k: (0, BLOCKS + first(k))),
            pl.BlockSpec((block, both), lambda k: (first(k), 0)),
            pl.BlockSpec((rows, block), lambda k: (0, 2 * BLOCKS + then(k))),
        ],
        out_specs=[
            pl.BlockSpec((rows, half), lambda k: (0, 0)),
            pl.BlockSpec((rows, half), lambda k: (0, 0)),
            pl.BlockSpec((block, half), lambda k: (then(k), 0)),
        ],
        out_shape=[
            jax.ShapeDtypeStruct((rows, half), F32),
            jax.ShapeDtypeStruct((rows, half), F32),
            pltpu.HBM((width, half), BF),
        ],
        scratch_shapes=[pltpu.VMEM((rows, both), F32), pltpu.VMEM((rows, half), BF)],
        compiler_params=pltpu.CompilerParams(
            dimension_semantics=("arbitrary",), vmem_limit_bytes=12 << 20
        ),
        cost_estimate=pl.CostEstimate(
            flops=6 * rows * width * half, transcendentals=rows * half, bytes_accessed=8 << 20
        ),
    )(tokens, whole, tokens)


def rest_kernel(
    row_ref, later_ref, cot_ref, weight_ref, gate_ref, up_ref, *others
):
    chunk_refs, (own_ref, other_ref) = others[:8], others[8:10]
    down_ref, sum_ref, grad_ref, hidden_ref, to_gate_ref, to_up_ref = others[10:]
    step = pl.program_id(0)
    half, lines = gate_ref.shape[1], down_ref.shape[0] // BLOCKS
    mine = own_ref.shape[1]

    @pl.when(step == 0)
    def _():
        sum_ref[...] = jnp.zeros_like(sum_ref)
        grad_ref[...] = jnp.zeros_like(grad_ref)
        for offset, chunk_ref in zip(OFFSETS, chunk_refs):
            at = (row_ref[0] + offset) & (len(OFFSETS) - 1)
            down_ref[:, pl.ds(at, 1)] = chunk_ref[...][:, None]

    @pl.when(step < BLOCKS)
    def _():
        down = down_ref[pl.ds(step * lines, lines)].reshape(-1, half)
        sum_ref[...] += jnp.dot(later_ref[...], weight_ref[...], preferred_element_type=F32)
        grad_ref[...] += jnp.dot(cot_ref[...], down, preferred_element_type=F32)

    @pl.when(step == BLOCKS - 1)
    def _():
        gate, up = sum_ref[:, :half], sum_ref[:, half:]
        hidden_ref[...] = (gate / (1.0 + jnp.exp(-gate)) * up).astype(BF)
        gate, grad = gate_ref[...], grad_ref[...]
        sig = 1.0 / (1.0 + jnp.exp(-gate))
        to_gate_ref[...] = (grad * up_ref[...] * sig * (1.0 + gate * (1.0 - sig))).astype(BF)
        to_up_ref[...] = (grad * (gate * sig)).astype(BF)

    @pl.when(step >= BLOCKS)
    def _():
        down = down_ref[pl.ds((step - BLOCKS) * lines, lines)].reshape(-1, half)
        out = dot_nt(hidden_ref[...], down)
        back = dot_nt(to_gate_ref[...], weight_ref[:, :half])
        back += dot_nt(to_up_ref[...], weight_ref[:, half:])
        own_ref[0], own_ref[1] = out[:mine], back[:mine]
        other_ref[0], other_ref[1] = out[mine:].astype(BF), back[mine:].astype(BF)


def rest_part(tokens, whole, gate_early, up_early, chunks):
    rows, (width, both) = tokens.shape[0], whole.shape
    block, half = width // BLOCKS, both // 2
    lines = chunks[0].shape[0]
    first = lambda k: jnp.minimum(k, BLOCKS - 1)
    then = lambda k: jnp.maximum(k - BLOCKS, 0)
    whole_of = lambda array: pl.BlockSpec(array.shape, lambda k: (0,) * array.ndim)
    out_block = pl.BlockSpec((2, rows // 2, block), lambda k: (0, 0, then(k)))
    return pl.pallas_call(
        rest_kernel,
        grid=(2 * BLOCKS,),
        in_specs=[
            pl.BlockSpec(memory_space=pltpu.SMEM),
            pl.BlockSpec((rows, block), lambda k: (0, first(k))),
            pl.BlockSpec((rows, block), lambda k: (0, 2 * BLOCKS + first(k))),
            pl.BlockSpec((block, both), lambda k: (k % BLOCKS, 0)),
            whole_of(gate_early),
            whole_of(up_early),
            *map(whole_of, chunks),
        ],
        out_specs=[out_block, out_block],
        out_shape=[
            jax.ShapeDtypeStruct((2, rows // 2, width), F32),
            jax.ShapeDtypeStruct((2, rows // 2, width), BF),
        ],
        scratch_shapes=[
            pltpu.VMEM((lines, len(chunks), *chunks[0].shape[1:]), BF),
            pltpu.VMEM((rows, both), F32),
            pltpu.VMEM((rows, half), F32),
            pltpu.VMEM((rows, half), BF),
            pltpu.VMEM((rows, half), BF),
            pltpu.VMEM((rows, half), BF),
        ],
        compiler_params=pltpu.CompilerParams(
            dimension_semantics=("arbitrary",), vmem_limit_bytes=16 << 20
        ),
        cost_estimate=pl.CostEstimate(
            flops=12 * rows * width * half, transcendentals=2 * rows * half, bytes_accessed=16 << 20
        ),
    )(
        lax.axis_index("y").astype(jnp.int32)[None],
        tokens,
        tokens,
        whole,
        gate_early,
        up_early,
        *chunks,
    )


def shards(later, early, cotangent, gate_w, up_w, down_w, down_grad_sum):
    rows, _ = later.shape
    line = spread(jnp.concatenate([gate_w, up_w], axis=1), "y")
    line = line.reshape(-1, line.shape[-1])
    whole = lax.all_gather(line, "z", axis=0, tiled=True)
    whole = pltpu.with_memory_space_constraint(whole, pltpu.HBM)
    tokens = jnp.concatenate([later, early, cotangent], axis=1)
    tokens = collect_tokens(tokens)
    chunks = gather_down(down_w)

    gate_early, up_early, down_grad = early_part(tokens, whole)
    received = lax.all_to_all(down_grad.reshape(-1, *gate_w.shape), FS, 0, 0)

    own, other = rest_part(tokens, whole, gate_early, up_early, chunks)
    later_output, earlier_grad_input = give_rows(own, other, rows)

    summed = jnp.sum(received.astype(F32), axis=0)
    factor = (rows * lax.axis_size(AXES)) ** (-0.5)
    return later_output, earlier_grad_input, down_grad_sum + summed * factor


def solution(mesh):
    split = Mesh(mesh.devices.reshape(8, 8, 4, 2), AXES)
    tokens, weights = P(AXES, None), P(FS, ("x", "c"))
    return jax.shard_map(
        shards,
        mesh=split,
        in_specs=(tokens,) * 3 + (weights,) * 4,
        out_specs=(tokens, tokens, weights),
        check_vma=False,
    )
```

```python
import jax
import jax.numpy as jnp
from jax import lax
from jax.experimental import pallas as pl
from jax.experimental.pallas import tpu as pltpu
from jax.sharding import Mesh
from jax.sharding import PartitionSpec as P


AXES = ("z", "y", "x", "c")
FS = ("z", "y")
STEPS = (0, 1, -1, 2)
BLOCKS = 4
OFFSETS = (0, -1, 1, -2, 2, -3, 3, 4)
BF, F32 = jnp.bfloat16, jnp.float32


def shift(value, axis, step):
    count = lax.axis_size(axis)
    if step == 0:
        return value
    return lax.ppermute(value, axis, [(i, (i + step) % count) for i in range(count)])


def copy_kernel(*refs):
    *ins, out_ref = refs
    at = 0
    for ref in ins:
        cols = ref.shape[1]
        out_ref[:, :, at : at + cols] = jnp.broadcast_to(ref[...], (out_ref.shape[0], *ref.shape))
        at += cols


def copies(count, *arrays):
    shape = (count, arrays[0].shape[0], sum(a.shape[1] for a in arrays))
    return pl.pallas_call(
        copy_kernel,
        out_shape=jax.ShapeDtypeStruct(shape, arrays[0].dtype),
        compiler_params=pltpu.CompilerParams(vmem_limit_bytes=8 << 20),
        cost_estimate=pl.CostEstimate(flops=1 << 20, transcendentals=0, bytes_accessed=1 << 20),
    )(*arrays)


def gather_down(down):
    fan = copies(lax.axis_size("z"), down)
    line = lax.all_to_all(fan, "z", 0, 0)
    chunks, ahead, behind = [line], line, line
    for _ in range(1, 4):
        ahead, behind = shift(ahead, "y", 1), shift(behind, "y", -1)
        chunks += [ahead, behind]
    return [*chunks, shift(ahead, "y", 1)]


def collect_tokens(own):
    pieces = [shift(own, "x", step) for step in STEPS]
    line = jnp.concatenate(pieces, axis=0)
    other = shift(line, "c", 1)
    return jnp.concatenate([line, other], axis=0)


def give_rows(own, other, rows):
    both = (own + shift(other, "c", 1).astype(F32)).astype(BF)
    total = 0.0
    for at, step in enumerate(STEPS):
        total += shift(both[:, at * rows : (at + 1) * rows], "x", -step).astype(F32)
    return total.astype(BF)


def dot_nt(leading, trailing):
    return lax.dot_general(
        leading, trailing, (((1,), (1,)), ((), ())), preferred_element_type=F32
    )


def early_kernel(token_ref, weight_ref, cot_ref, gate_ref, up_ref, grad_ref, sum_ref, hidden_ref):
    step = pl.program_id(0)
    half = gate_ref.shape[1]

    @pl.when(step == 0)
    def _():
        sum_ref[...] = jnp.zeros_like(sum_ref)

    @pl.when(step < BLOCKS)
    def _():
        sum_ref[...] += jnp.dot(token_ref[...], weight_ref[...], preferred_element_type=F32)

    @pl.when(step == BLOCKS - 1)
    def _():
        gate, up = sum_ref[:, :half], sum_ref[:, half:]
        gate_ref[...] = gate
        up_ref[...] = up
        hidden_ref[...] = (gate / (1.0 + jnp.exp(-gate)) * up).astype(BF)

    @pl.when(step >= BLOCKS)
    def _():
        grad_ref[...] = lax.dot_general(
            cot_ref[...], hidden_ref[...], (((0,), (0,)), ((), ())), preferred_element_type=F32
        ).astype(BF)


def early_part(tokens, whole):
    rows, width = tokens.shape[0], whole.shape[0]
    both, block = whole.shape[1], width // BLOCKS
    half = both // 2
    first = lambda k: jnp.minimum(k, BLOCKS - 1)
    then = lambda k: jnp.maximum(k - BLOCKS, 0)
    return pl.pallas_call(
        early_kernel,
        grid=(2 * BLOCKS,),
        in_specs=[
            pl.BlockSpec((rows, block), lambda k: (0, BLOCKS + first(k))),
            pl.BlockSpec((block, both), lambda k: (first(k), 0)),
            pl.BlockSpec((rows, block), lambda k: (0, 2 * BLOCKS + then(k))),
        ],
        out_specs=[
            pl.BlockSpec((rows, half), lambda k: (0, 0)),
            pl.BlockSpec((rows, half), lambda k: (0, 0)),
            pl.BlockSpec((block, half), lambda k: (then(k), 0)),
        ],
        out_shape=[
            jax.ShapeDtypeStruct((rows, half), F32),
            jax.ShapeDtypeStruct((rows, half), F32),
            pltpu.HBM((width, half), BF),
        ],
        scratch_shapes=[pltpu.VMEM((rows, both), F32), pltpu.VMEM((rows, half), BF)],
        compiler_params=pltpu.CompilerParams(
            dimension_semantics=("arbitrary",), vmem_limit_bytes=12 << 20
        ),
        cost_estimate=pl.CostEstimate(
            flops=6 * rows * width * half, transcendentals=rows * half, bytes_accessed=8 << 20
        ),
    )(tokens, whole, tokens)


def rest_kernel(
    row_ref, later_ref, cot_ref, weight_ref, gate_ref, up_ref, *others
):
    chunk_refs, (own_ref, other_ref) = others[:8], others[8:10]
    down_ref, sum_ref, grad_ref, hidden_ref, to_gate_ref, to_up_ref = others[10:]
    step = pl.program_id(0)
    half, lines = gate_ref.shape[1], down_ref.shape[0] // BLOCKS
    mine = own_ref.shape[1]

    @pl.when(step == 0)
    def _():
        sum_ref[...] = jnp.zeros_like(sum_ref)
        grad_ref[...] = jnp.zeros_like(grad_ref)
        for offset, chunk_ref in zip(OFFSETS, chunk_refs):
            at = (row_ref[0] + offset) & (len(OFFSETS) - 1)
            down_ref[:, pl.ds(at, 1)] = chunk_ref[...][:, None]

    @pl.when(step < BLOCKS)
    def _():
        down = down_ref[pl.ds(step * lines, lines)].reshape(-1, half)
        sum_ref[...] += jnp.dot(later_ref[...], weight_ref[...], preferred_element_type=F32)
        grad_ref[...] += jnp.dot(cot_ref[...], down, preferred_element_type=F32)

    @pl.when(step == BLOCKS - 1)
    def _():
        gate, up = sum_ref[:, :half], sum_ref[:, half:]
        hidden_ref[...] = (gate / (1.0 + jnp.exp(-gate)) * up).astype(BF)
        gate, grad = gate_ref[...], grad_ref[...]
        sig = 1.0 / (1.0 + jnp.exp(-gate))
        to_gate_ref[...] = (grad * up_ref[...] * sig * (1.0 + gate * (1.0 - sig))).astype(BF)
        to_up_ref[...] = (grad * (gate * sig)).astype(BF)

    @pl.when(step >= BLOCKS)
    def _():
        down = down_ref[pl.ds((step - BLOCKS) * lines, lines)].reshape(-1, half)
        out = dot_nt(hidden_ref[...], down)
        back = dot_nt(to_gate_ref[...], weight_ref[:, :half])
        back += dot_nt(to_up_ref[...], weight_ref[:, half:])
        own_ref[0], own_ref[1] = out[:mine], back[:mine]
        other_ref[0], other_ref[1] = out[mine:].astype(BF), back[mine:].astype(BF)


def rest_part(tokens, whole, gate_early, up_early, chunks):
    rows, (width, both) = tokens.shape[0], whole.shape
    block, half = width // BLOCKS, both // 2
    lines = chunks[0].shape[0]
    first = lambda k: jnp.minimum(k, BLOCKS - 1)
    then = lambda k: jnp.maximum(k - BLOCKS, 0)
    whole_of = lambda array: pl.BlockSpec(array.shape, lambda k: (0,) * array.ndim)
    out_block = pl.BlockSpec((2, rows // 2, block), lambda k: (0, 0, then(k)))
    return pl.pallas_call(
        rest_kernel,
        grid=(2 * BLOCKS,),
        in_specs=[
            pl.BlockSpec(memory_space=pltpu.SMEM),
            pl.BlockSpec((rows, block), lambda k: (0, first(k))),
            pl.BlockSpec((rows, block), lambda k: (0, 2 * BLOCKS + first(k))),
            pl.BlockSpec((block, both), lambda k: (k % BLOCKS, 0)),
            whole_of(gate_early),
            whole_of(up_early),
            *map(whole_of, chunks),
        ],
        out_specs=[out_block, out_block],
        out_shape=[
            jax.ShapeDtypeStruct((2, rows // 2, width), F32),
            jax.ShapeDtypeStruct((2, rows // 2, width), BF),
        ],
        scratch_shapes=[
            pltpu.VMEM((lines, len(chunks), *chunks[0].shape[1:]), BF),
            pltpu.VMEM((rows, both), F32),
            pltpu.VMEM((rows, half), F32),
            pltpu.VMEM((rows, half), BF),
            pltpu.VMEM((rows, half), BF),
            pltpu.VMEM((rows, half), BF),
        ],
        compiler_params=pltpu.CompilerParams(
            dimension_semantics=("arbitrary",), vmem_limit_bytes=16 << 20
        ),
        cost_estimate=pl.CostEstimate(
            flops=12 * rows * width * half, transcendentals=2 * rows * half, bytes_accessed=16 << 20
        ),
    )(
        lax.axis_index("y").astype(jnp.int32)[None],
        tokens,
        tokens,
        whole,
        gate_early,
        up_early,
        *chunks,
    )


def shards(later, early, cotangent, gate_w, up_w, down_w, down_grad_sum):
    rows, _ = later.shape
    fan = copies(lax.axis_size("y"), gate_w, up_w)
    line = lax.all_to_all(fan, "y", 0, 0)
    line = line.reshape(-1, line.shape[-1])
    whole = lax.all_gather(line, "z", axis=0, tiled=True)
    whole = pltpu.with_memory_space_constraint(whole, pltpu.HBM)
    tokens = copies(1, later, early, cotangent)[0]
    tokens = collect_tokens(tokens)
    tokens = pltpu.with_memory_space_constraint(tokens, pltpu.VMEM)
    chunks = gather_down(down_w)

    gate_early, up_early, down_grad = early_part(tokens, whole)
    received = lax.all_to_all(down_grad.reshape(-1, *gate_w.shape), FS, 0, 0)

    own, other = rest_part(tokens, whole, gate_early, up_early, chunks)
    later_output, earlier_grad_input = give_rows(own, other, rows)

    summed = jnp.sum(received.astype(F32), axis=0)
    factor = (rows * lax.axis_size(AXES)) ** (-0.5)
    return later_output, earlier_grad_input, down_grad_sum + summed * factor


def solution(mesh):
    split = Mesh(mesh.devices.reshape(8, 8, 4, 2), AXES)
    tokens, weights = P(AXES, None), P(FS, ("x", "c"))
    return jax.shard_map(
        shards,
        mesh=split,
        in_specs=(tokens,) * 3 + (weights,) * 4,
        out_specs=(tokens, tokens, weights),
        check_vma=False,
    )
```

```python
import jax
import jax.numpy as jnp
from jax import lax
from jax.experimental import pallas as pl
from jax.experimental.pallas import tpu as pltpu
from jax.sharding import Mesh
from jax.sharding import PartitionSpec as P


AXES = ("z", "y", "x", "c")
FS = ("z", "y")
STEPS = (0, 1, -1, 2)
BLOCKS = 4
OFFSETS = (0, -1, 1, -2, 2, -3, 3, 4)
BF, F32 = jnp.bfloat16, jnp.float32


def shift(value, axis, step):
    count = lax.axis_size(axis)
    if step == 0:
        return value
    return lax.ppermute(value, axis, [(i, (i + step) % count) for i in range(count)])


def copy_kernel(*refs):
    *ins, out_ref = refs
    at = 0
    for ref in ins:
        cols = ref.shape[1]
        out_ref[:, :, at : at + cols] = jnp.broadcast_to(ref[...], (out_ref.shape[0], *ref.shape))
        at += cols


def copies(count, *arrays):
    shape = (count, arrays[0].shape[0], sum(a.shape[1] for a in arrays))
    return pl.pallas_call(
        copy_kernel,
        out_shape=jax.ShapeDtypeStruct(shape, arrays[0].dtype),
        compiler_params=pltpu.CompilerParams(vmem_limit_bytes=8 << 20),
        cost_estimate=pl.CostEstimate(flops=1 << 20, transcendentals=0, bytes_accessed=1 << 20),
    )(*arrays)


def stack_kernel(*refs):
    *ins, out_ref = refs
    for at, ref in enumerate(ins):
        rows = ref.shape[0]
        out_ref[at * rows : (at + 1) * rows] = ref[...]


def stacked(pieces):
    rows, cols = pieces[0].shape
    return pl.pallas_call(
        stack_kernel,
        out_shape=jax.ShapeDtypeStruct((len(pieces) * rows, cols), pieces[0].dtype),
        compiler_params=pltpu.CompilerParams(vmem_limit_bytes=8 << 20),
        cost_estimate=pl.CostEstimate(flops=1 << 20, transcendentals=0, bytes_accessed=1 << 20),
    )(*pieces)


def gather_down(down):
    fan = copies(lax.axis_size("z"), down)
    line = lax.all_to_all(fan, "z", 0, 0)
    chunks, ahead, behind = [line], line, line
    for _ in range(1, 4):
        ahead, behind = shift(ahead, "y", 1), shift(behind, "y", -1)
        chunks += [ahead, behind]
    return [*chunks, shift(ahead, "y", 1)]


def collect_tokens(own):
    pieces = [shift(own, "x", step) for step in STEPS]
    line = stacked(pieces)
    other = shift(line, "c", 1)
    return line, other


def give_rows(own, other, rows):
    both = (own + shift(other, "c", 1).astype(F32)).astype(BF)
    total = 0.0
    for at, step in enumerate(STEPS):
        total += shift(both[:, at * rows : (at + 1) * rows], "x", -step).astype(F32)
    return total.astype(BF)


def dot_nt(leading, trailing):
    return lax.dot_general(
        leading, trailing, (((1,), (1,)), ((), ())), preferred_element_type=F32
    )


def rows_of(refs):
    return jnp.concatenate([ref[...] for ref in refs], axis=0)


def early_kernel(
    own_ref, far_ref, weight_ref, cot_ref, cot_far_ref, gate_ref, up_ref, grad_ref, sum_ref, hidden_ref
):
    step = pl.program_id(0)
    half = gate_ref.shape[1]

    @pl.when(step == 0)
    def _():
        sum_ref[...] = jnp.zeros_like(sum_ref)

    @pl.when(step < BLOCKS)
    def _():
        block = rows_of((own_ref, far_ref))
        sum_ref[...] += jnp.dot(block, weight_ref[...], preferred_element_type=F32)

    @pl.when(step == BLOCKS - 1)
    def _():
        gate, up = sum_ref[:, :half], sum_ref[:, half:]
        gate_ref[...] = gate
        up_ref[...] = up
        hidden_ref[...] = (gate / (1.0 + jnp.exp(-gate)) * up).astype(BF)

    @pl.when(step >= BLOCKS)
    def _():
        grad_ref[...] = lax.dot_general(
            rows_of((cot_ref, cot_far_ref)), hidden_ref[...], (((0,), (0,)), ((), ())), preferred_element_type=F32
        ).astype(BF)


def early_part(tokens, whole):
    mine, width = tokens[0].shape[0], whole.shape[0]
    rows = 2 * mine
    both, block = whole.shape[1], width // BLOCKS
    half = both // 2
    first = lambda k: jnp.minimum(k, BLOCKS - 1)
    then = lambda k: jnp.maximum(k - BLOCKS, 0)
    return pl.pallas_call(
        early_kernel,
        grid=(2 * BLOCKS,),
        in_specs=[
            *[pl.BlockSpec((mine, block), lambda k: (0, BLOCKS + first(k)))] * 2,
            pl.BlockSpec((block, both), lambda k: (first(k), 0)),
            *[pl.BlockSpec((mine, block), lambda k: (0, 2 * BLOCKS + then(k)))] * 2,
        ],
        out_specs=[
            pl.BlockSpec((rows, half), lambda k: (0, 0)),
            pl.BlockSpec((rows, half), lambda k: (0, 0)),
            pl.BlockSpec((block, half), lambda k: (then(k), 0)),
        ],
        out_shape=[
            jax.ShapeDtypeStruct((rows, half), F32),
            jax.ShapeDtypeStruct((rows, half), F32),
            pltpu.HBM((width, half), BF),
        ],
        scratch_shapes=[pltpu.VMEM((rows, both), F32), pltpu.VMEM((rows, half), BF)],
        compiler_params=pltpu.CompilerParams(
            dimension_semantics=("arbitrary",), vmem_limit_bytes=12 << 20
        ),
        cost_estimate=pl.CostEstimate(
            flops=6 * rows * width * half, transcendentals=rows * half, bytes_accessed=8 << 20
        ),
    )(*tokens, whole, *tokens)


def rest_kernel(
    row_ref, own_in_ref, far_in_ref, cot_ref, cot_far_ref, weight_ref, gate_ref, up_ref, *others
):
    chunk_refs, (own_ref, other_ref) = others[:8], others[8:10]
    down_ref, sum_ref, grad_ref, hidden_ref, to_gate_ref, to_up_ref = others[10:]
    step = pl.program_id(0)
    half, lines = gate_ref.shape[1], down_ref.shape[0] // BLOCKS
    mine = own_ref.shape[1]

    @pl.when(step == 0)
    def _():
        sum_ref[...] = jnp.zeros_like(sum_ref)
        grad_ref[...] = jnp.zeros_like(grad_ref)
        for offset, chunk_ref in zip(OFFSETS, chunk_refs):
            at = (row_ref[0] + offset) & (len(OFFSETS) - 1)
            down_ref[:, pl.ds(at, 1)] = chunk_ref[...][:, None]

    @pl.when(step < BLOCKS)
    def _():
        down = down_ref[pl.ds(step * lines, lines)].reshape(-1, half)
        block = rows_of((own_in_ref, far_in_ref))
        sum_ref[...] += jnp.dot(block, weight_ref[...], preferred_element_type=F32)
        cot = rows_of((cot_ref, cot_far_ref))
        grad_ref[...] += jnp.dot(cot, down, preferred_element_type=F32)

    @pl.when(step == BLOCKS - 1)
    def _():
        gate, up = sum_ref[:, :half], sum_ref[:, half:]
        hidden_ref[...] = (gate / (1.0 + jnp.exp(-gate)) * up).astype(BF)
        gate, grad = gate_ref[...], grad_ref[...]
        sig = 1.0 / (1.0 + jnp.exp(-gate))
        to_gate_ref[...] = (grad * up_ref[...] * sig * (1.0 + gate * (1.0 - sig))).astype(BF)
        to_up_ref[...] = (grad * (gate * sig)).astype(BF)

    @pl.when(step >= BLOCKS)
    def _():
        down = down_ref[pl.ds((step - BLOCKS) * lines, lines)].reshape(-1, half)
        out = dot_nt(hidden_ref[...], down)
        back = dot_nt(to_gate_ref[...], weight_ref[:, :half])
        back += dot_nt(to_up_ref[...], weight_ref[:, half:])
        own_ref[0], own_ref[1] = out[:mine], back[:mine]
        other_ref[0], other_ref[1] = out[mine:].astype(BF), back[mine:].astype(BF)


def rest_part(tokens, whole, gate_early, up_early, chunks):
    mine, (width, both) = tokens[0].shape[0], whole.shape
    rows = 2 * mine
    block, half = width // BLOCKS, both // 2
    lines = chunks[0].shape[0]
    first = lambda k: jnp.minimum(k, BLOCKS - 1)
    then = lambda k: jnp.maximum(k - BLOCKS, 0)
    whole_of = lambda array: pl.BlockSpec(array.shape, lambda k: (0,) * array.ndim)
    out_block = pl.BlockSpec((2, rows // 2, block), lambda k: (0, 0, then(k)))
    return pl.pallas_call(
        rest_kernel,
        grid=(2 * BLOCKS,),
        in_specs=[
            pl.BlockSpec(memory_space=pltpu.SMEM),
            *[pl.BlockSpec((mine, block), lambda k: (0, first(k)))] * 2,
            *[pl.BlockSpec((mine, block), lambda k: (0, 2 * BLOCKS + first(k)))] * 2,
            pl.BlockSpec((block, both), lambda k: (k % BLOCKS, 0)),
            whole_of(gate_early),
            whole_of(up_early),
            *map(whole_of, chunks),
        ],
        out_specs=[out_block, out_block],
        out_shape=[
            jax.ShapeDtypeStruct((2, rows // 2, width), F32),
            jax.ShapeDtypeStruct((2, rows // 2, width), BF),
        ],
        scratch_shapes=[
            pltpu.VMEM((lines, len(chunks), *chunks[0].shape[1:]), BF),
            pltpu.VMEM((rows, both), F32),
            pltpu.VMEM((rows, half), F32),
            pltpu.VMEM((rows, half), BF),
            pltpu.VMEM((rows, half), BF),
            pltpu.VMEM((rows, half), BF),
        ],
        compiler_params=pltpu.CompilerParams(
            dimension_semantics=("arbitrary",), vmem_limit_bytes=16 << 20
        ),
        cost_estimate=pl.CostEstimate(
            flops=12 * rows * width * half, transcendentals=2 * rows * half, bytes_accessed=16 << 20
        ),
    )(
        lax.axis_index("y").astype(jnp.int32)[None],
        *tokens,
        *tokens,
        whole,
        gate_early,
        up_early,
        *chunks,
    )


def shards(later, early, cotangent, gate_w, up_w, down_w, down_grad_sum):
    rows, _ = later.shape
    fan = copies(lax.axis_size("y"), gate_w, up_w)
    line = lax.all_to_all(fan, "y", 0, 0)
    line = line.reshape(-1, line.shape[-1])
    whole = lax.all_gather(line, "z", axis=0, tiled=True)
    whole = pltpu.with_memory_space_constraint(whole, pltpu.HBM)
    tokens = copies(1, later, early, cotangent)[0]
    tokens = collect_tokens(tokens)
    tokens = [pltpu.with_memory_space_constraint(t, pltpu.VMEM) for t in tokens]
    chunks = gather_down(down_w)

    gate_early, up_early, down_grad = early_part(tokens, whole)
    received = lax.all_to_all(down_grad.reshape(-1, *gate_w.shape), FS, 0, 0)

    own, other = rest_part(tokens, whole, gate_early, up_early, chunks)
    later_output, earlier_grad_input = give_rows(own, other, rows)

    summed = jnp.sum(received.astype(F32), axis=0)
    factor = (rows * lax.axis_size(AXES)) ** (-0.5)
    return later_output, earlier_grad_input, down_grad_sum + summed * factor


def solution(mesh):
    split = Mesh(mesh.devices.reshape(8, 8, 4, 2), AXES)
    tokens, weights = P(AXES, None), P(FS, ("x", "c"))
    return jax.shard_map(
        shards,
        mesh=split,
        in_specs=(tokens,) * 3 + (weights,) * 4,
        out_specs=(tokens, tokens, weights),
        check_vma=False,
    )
```

```python
import jax
import jax.numpy as jnp
from jax import lax
from jax.experimental import pallas as pl
from jax.experimental.pallas import tpu as pltpu
from jax.sharding import Mesh
from jax.sharding import PartitionSpec as P


AXES = ("z", "y", "x", "c")
FS = ("z", "y")
STEPS = (0, 1, -1, 2)
BLOCKS = 4
OFFSETS = (0, -1, 1, -2, 2, -3, 3, 4)
BF, F32 = jnp.bfloat16, jnp.float32


def shift(value, axis, step):
    count = lax.axis_size(axis)
    if step == 0:
        return value
    return lax.ppermute(value, axis, [(i, (i + step) % count) for i in range(count)])


def copy_kernel(*refs):
    *ins, out_ref = refs
    at = 0
    for ref in ins:
        cols = ref.shape[1]
        out_ref[:, :, at : at + cols] = jnp.broadcast_to(ref[...], (out_ref.shape[0], *ref.shape))
        at += cols


def copies(count, *arrays):
    shape = (count, arrays[0].shape[0], sum(a.shape[1] for a in arrays))
    return pl.pallas_call(
        copy_kernel,
        out_shape=jax.ShapeDtypeStruct(shape, arrays[0].dtype),
        compiler_params=pltpu.CompilerParams(vmem_limit_bytes=8 << 20),
        cost_estimate=pl.CostEstimate(flops=1 << 20, transcendentals=0, bytes_accessed=1 << 20),
    )(*[pltpu.with_memory_space_constraint(a, pltpu.HBM) for a in arrays])


def stack_kernel(*refs):
    *ins, out_ref = refs
    for at, ref in enumerate(ins):
        rows = ref.shape[0]
        out_ref[at * rows : (at + 1) * rows] = ref[...]


def stacked(pieces):
    rows, cols = pieces[0].shape
    return pl.pallas_call(
        stack_kernel,
        out_shape=jax.ShapeDtypeStruct((len(pieces) * rows, cols), pieces[0].dtype),
        compiler_params=pltpu.CompilerParams(vmem_limit_bytes=8 << 20),
        cost_estimate=pl.CostEstimate(flops=1 << 20, transcendentals=0, bytes_accessed=1 << 20),
    )(*pieces)


def gather_down(down):
    fan = copies(lax.axis_size("z"), down)
    line = lax.all_to_all(fan, "z", 0, 0)
    chunks, ahead, behind = [line], line, line
    for _ in range(1, 4):
        ahead, behind = shift(ahead, "y", 1), shift(behind, "y", -1)
        chunks += [ahead, behind]
    return [*chunks, shift(ahead, "y", 1)]


def collect_tokens(own):
    pieces = [shift(own, "x", step) for step in STEPS]
    line = stacked(pieces)
    other = shift(line, "c", 1)
    return line, other


def give_rows(own, other, rows):
    both = (own + shift(other, "c", 1).astype(F32)).astype(BF)
    total = 0.0
    for at, step in enumerate(STEPS):
        total += shift(both[:, at * rows : (at + 1) * rows], "x", -step).astype(F32)
    return total.astype(BF)


def dot_nt(leading, trailing):
    return lax.dot_general(
        leading, trailing, (((1,), (1,)), ((), ())), preferred_element_type=F32
    )


def rows_of(refs):
    return jnp.concatenate([ref[...] for ref in refs], axis=0)


def early_kernel(
    own_ref, far_ref, whole_ref, gate_ref, up_ref, out_ref,
    weight_ref, token_ref, cot_ref, grad_ref, in_sems, out_sems,
):
    blocks, block, _ = weight_ref.shape
    mine, half, width = own_ref.shape[0], gate_ref.shape[1], token_ref.shape[1]
    rows = lambda k: pl.ds(k * block, block)
    loads = [
        pltpu.make_async_copy(whole_ref.at[rows(k)], weight_ref.at[k], in_sems.at[k])
        for k in range(blocks)
    ]
    stores = [
        pltpu.make_async_copy(grad_ref.at[k], out_ref.at[rows(k)], out_sems.at[k])
        for k in range(blocks)
    ]
    for load in loads:
        load.start()
    for at, ref in ((0, own_ref), (mine, far_ref)):
        token_ref[at : at + mine] = ref[:, width : 2 * width]
        cot_ref[at : at + mine] = ref[:, 2 * width :]
    both = 0.0
    for k in range(blocks):
        loads[k].wait()
        both += jnp.dot(token_ref[:, rows(k)], weight_ref[k], preferred_element_type=F32)
    gate, up = both[:, :half], both[:, half:]
    gate_ref[...] = gate
    up_ref[...] = up
    hidden = (gate / (1.0 + jnp.exp(-gate)) * up).astype(BF)
    for k in range(blocks):
        grad_ref[k] = lax.dot_general(
            cot_ref[:, rows(k)], hidden, (((0,), (0,)), ((), ())), preferred_element_type=F32
        ).astype(BF)
        stores[k].start()
    for store in stores:
        store.wait()


def early_part(tokens, whole):
    rows, width = 2 * tokens[0].shape[0], whole.shape[0]
    both, block = whole.shape[1], width // BLOCKS
    half = both // 2
    vmem, hbm = pl.BlockSpec(memory_space=pltpu.VMEM), pl.BlockSpec(memory_space=pltpu.HBM)
    return pl.pallas_call(
        early_kernel,
        in_specs=[vmem, vmem, hbm],
        out_specs=[vmem, vmem, hbm],
        out_shape=[
            jax.ShapeDtypeStruct((rows, half), F32),
            jax.ShapeDtypeStruct((rows, half), F32),
            pltpu.HBM((width, half), BF),
        ],
        scratch_shapes=[
            pltpu.VMEM((BLOCKS, block, both), BF),
            pltpu.VMEM((rows, width), BF),
            pltpu.VMEM((rows, width), BF),
            pltpu.VMEM((BLOCKS, block, half), BF),
            pltpu.SemaphoreType.DMA((BLOCKS,)),
            pltpu.SemaphoreType.DMA((BLOCKS,)),
        ],
        compiler_params=pltpu.CompilerParams(vmem_limit_bytes=16 << 20),
        cost_estimate=pl.CostEstimate(
            flops=6 * rows * width * half, transcendentals=rows * half, bytes_accessed=8 << 20
        ),
    )(*tokens, whole)


def rest_kernel(
    row_ref, own_in_ref, far_in_ref, cot_ref, cot_far_ref, weight_ref, gate_ref, up_ref, *others
):
    chunk_refs, (own_ref, other_ref) = others[:8], others[8:10]
    down_ref, sum_ref, grad_ref, hidden_ref, to_gate_ref, to_up_ref = others[10:]
    step = pl.program_id(0)
    half, lines = gate_ref.shape[1], down_ref.shape[0] // BLOCKS
    mine = own_ref.shape[1]

    @pl.when(step == 0)
    def _():
        sum_ref[...] = jnp.zeros_like(sum_ref)
        grad_ref[...] = jnp.zeros_like(grad_ref)
        for offset, chunk_ref in zip(OFFSETS, chunk_refs):
            at = (row_ref[0] + offset) & (len(OFFSETS) - 1)
            down_ref[:, pl.ds(at, 1)] = chunk_ref[...][:, None]

    @pl.when(step < BLOCKS)
    def _():
        down = down_ref[pl.ds(step * lines, lines)].reshape(-1, half)
        block = rows_of((own_in_ref, far_in_ref))
        sum_ref[...] += jnp.dot(block, weight_ref[...], preferred_element_type=F32)
        cot = rows_of((cot_ref, cot_far_ref))
        grad_ref[...] += jnp.dot(cot, down, preferred_element_type=F32)

    @pl.when(step == BLOCKS - 1)
    def _():
        gate, up = sum_ref[:, :half], sum_ref[:, half:]
        hidden_ref[...] = (gate / (1.0 + jnp.exp(-gate)) * up).astype(BF)
        gate, grad = gate_ref[...], grad_ref[...]
        sig = 1.0 / (1.0 + jnp.exp(-gate))
        to_gate_ref[...] = (grad * up_ref[...] * sig * (1.0 + gate * (1.0 - sig))).astype(BF)
        to_up_ref[...] = (grad * (gate * sig)).astype(BF)

    @pl.when(step >= BLOCKS)
    def _():
        down = down_ref[pl.ds((step - BLOCKS) * lines, lines)].reshape(-1, half)
        out = dot_nt(hidden_ref[...], down)
        back = dot_nt(to_gate_ref[...], weight_ref[:, :half])
        back += dot_nt(to_up_ref[...], weight_ref[:, half:])
        own_ref[0], own_ref[1] = out[:mine], back[:mine]
        other_ref[0], other_ref[1] = out[mine:].astype(BF), back[mine:].astype(BF)


def rest_part(tokens, whole, gate_early, up_early, chunks):
    mine, (width, both) = tokens[0].shape[0], whole.shape
    rows = 2 * mine
    block, half = width // BLOCKS, both // 2
    lines = chunks[0].shape[0]
    first = lambda k: jnp.minimum(k, BLOCKS - 1)
    then = lambda k: jnp.maximum(k - BLOCKS, 0)
    whole_of = lambda array: pl.BlockSpec(array.shape, lambda k: (0,) * array.ndim)
    out_block = pl.BlockSpec((2, rows // 2, block), lambda k: (0, 0, then(k)))
    return pl.pallas_call(
        rest_kernel,
        grid=(2 * BLOCKS,),
        in_specs=[
            pl.BlockSpec(memory_space=pltpu.SMEM),
            *[pl.BlockSpec((mine, block), lambda k: (0, first(k)))] * 2,
            *[pl.BlockSpec((mine, block), lambda k: (0, 2 * BLOCKS + first(k)))] * 2,
            pl.BlockSpec((block, both), lambda k: (k % BLOCKS, 0)),
            whole_of(gate_early),
            whole_of(up_early),
            *map(whole_of, chunks),
        ],
        out_specs=[out_block, out_block],
        out_shape=[
            jax.ShapeDtypeStruct((2, rows // 2, width), F32),
            jax.ShapeDtypeStruct((2, rows // 2, width), BF),
        ],
        scratch_shapes=[
            pltpu.VMEM((lines, len(chunks), *chunks[0].shape[1:]), BF),
            pltpu.VMEM((rows, both), F32),
            pltpu.VMEM((rows, half), F32),
            pltpu.VMEM((rows, half), BF),
            pltpu.VMEM((rows, half), BF),
            pltpu.VMEM((rows, half), BF),
        ],
        compiler_params=pltpu.CompilerParams(
            dimension_semantics=("arbitrary",), vmem_limit_bytes=16 << 20
        ),
        cost_estimate=pl.CostEstimate(
            flops=12 * rows * width * half, transcendentals=2 * rows * half, bytes_accessed=16 << 20
        ),
    )(
        lax.axis_index("y").astype(jnp.int32)[None],
        *tokens,
        *tokens,
        whole,
        gate_early,
        up_early,
        *chunks,
    )


def shards(later, early, cotangent, gate_w, up_w, down_w, down_grad_sum):
    rows, _ = later.shape
    fan = copies(lax.axis_size("y"), gate_w, up_w)
    line = lax.all_to_all(fan, "y", 0, 0)
    line = line.reshape(-1, line.shape[-1])
    whole = lax.all_gather(line, "z", axis=0, tiled=True)
    whole = pltpu.with_memory_space_constraint(whole, pltpu.HBM)
    tokens = copies(1, later, early, cotangent)[0]
    tokens = collect_tokens(tokens)
    tokens = [pltpu.with_memory_space_constraint(t, pltpu.VMEM) for t in tokens]
    chunks = gather_down(down_w)

    gate_early, up_early, down_grad = early_part(tokens, whole)
    received = lax.all_to_all(down_grad.reshape(-1, *gate_w.shape), FS, 0, 0)

    own, other = rest_part(tokens, whole, gate_early, up_early, chunks)
    later_output, earlier_grad_input = give_rows(own, other, rows)

    summed = jnp.sum(received.astype(F32), axis=0)
    factor = (rows * lax.axis_size(AXES)) ** (-0.5)
    return later_output, earlier_grad_input, down_grad_sum + summed * factor


def solution(mesh):
    split = Mesh(mesh.devices.reshape(8, 8, 4, 2), AXES)
    tokens, weights = P(AXES, None), P(FS, ("x", "c"))
    return jax.shard_map(
        shards,
        mesh=split,
        in_specs=(tokens,) * 3 + (weights,) * 4,
        out_specs=(tokens, tokens, weights),
        check_vma=False,
    )
```

```python
import functools

import jax
import jax.numpy as jnp
from jax import lax
from jax.experimental import pallas as pl
from jax.experimental.pallas import tpu as pltpu
from jax.sharding import Mesh
from jax.sharding import PartitionSpec as P


AXES = ("z", "y", "x", "c")
FS = ("z", "y")
STEPS = (0, 1, -1, 2)
BLOCKS = 4
OFFSETS = (0, -1, 1, -2, 2, -3, 3, 4)
BF, F32 = jnp.bfloat16, jnp.float32


def shift(value, axis, step):
    count = lax.axis_size(axis)
    if step == 0:
        return value
    return lax.ppermute(value, axis, [(i, (i + step) % count) for i in range(count)])


def copy_kernel(*refs):
    *ins, out_ref = refs
    at = 0
    for ref in ins:
        cols = ref.shape[1]
        out_ref[:, :, at : at + cols] = jnp.broadcast_to(ref[...], (out_ref.shape[0], *ref.shape))
        at += cols


def copies(count, *arrays):
    shape = (count, arrays[0].shape[0], sum(a.shape[1] for a in arrays))
    return pl.pallas_call(
        copy_kernel,
        out_shape=jax.ShapeDtypeStruct(shape, arrays[0].dtype),
        compiler_params=pltpu.CompilerParams(vmem_limit_bytes=8 << 20),
        cost_estimate=pl.CostEstimate(flops=1 << 20, transcendentals=0, bytes_accessed=1 << 20),
    )(*[pltpu.with_memory_space_constraint(a, pltpu.HBM) for a in arrays])


def fan_kernel(*refs):
    *ins, out_ref, sems = refs
    moves, at = [], 0
    for ref in ins:
        cols = ref.shape[1]
        for k in range(out_ref.shape[0]):
            place = out_ref.at[k, :, pl.ds(at, cols)]
            moves.append(pltpu.make_async_copy(ref, place, sems.at[len(moves)]))
        at += cols
    for move in moves:
        move.start()
    for move in moves:
        move.wait()


def fanned(count, *arrays):
    shape = (count, arrays[0].shape[0], sum(a.shape[1] for a in arrays))
    hbm = pl.BlockSpec(memory_space=pltpu.HBM)
    return pl.pallas_call(
        fan_kernel,
        in_specs=[hbm] * len(arrays),
        out_specs=hbm,
        out_shape=pltpu.HBM(shape, arrays[0].dtype),
        scratch_shapes=[pltpu.SemaphoreType.DMA((count * len(arrays),))],
        compiler_params=pltpu.CompilerParams(vmem_limit_bytes=1 << 20),
        cost_estimate=pl.CostEstimate(flops=1 << 20, transcendentals=0, bytes_accessed=1 << 20),
    )(*[pltpu.with_memory_space_constraint(a, pltpu.HBM) for a in arrays])


def stack_kernel(*refs):
    *ins, out_ref = refs
    for at, ref in enumerate(ins):
        rows = ref.shape[0]
        out_ref[at * rows : (at + 1) * rows] = ref[...]


def stacked(pieces):
    rows, cols = pieces[0].shape
    return pl.pallas_call(
        stack_kernel,
        out_shape=jax.ShapeDtypeStruct((len(pieces) * rows, cols), pieces[0].dtype),
        compiler_params=pltpu.CompilerParams(vmem_limit_bytes=8 << 20),
        cost_estimate=pl.CostEstimate(flops=1 << 20, transcendentals=0, bytes_accessed=1 << 20),
    )(*pieces)


def gather_down(down):
    fan = fanned(lax.axis_size("z"), down)
    line = lax.all_to_all(fan, "z", 0, 0)
    chunks, ahead, behind = [line], line, line
    for _ in range(1, 4):
        ahead, behind = shift(ahead, "y", 1), shift(behind, "y", -1)
        chunks += [ahead, behind]
    return [*chunks, shift(ahead, "y", 1)]


def collect_tokens(own):
    pieces = [shift(own, "x", step) for step in STEPS]
    line = stacked(pieces)
    other = shift(line, "c", 1)
    return line, other


def give_rows(own, other, rows):
    both = (own + shift(other, "c", 1).astype(F32)).astype(BF)
    total = 0.0
    for at, step in enumerate(STEPS):
        total += shift(both[:, at * rows : (at + 1) * rows], "x", -step).astype(F32)
    return total.astype(BF)


def dot_nt(leading, trailing):
    return lax.dot_general(
        leading, trailing, (((1,), (1,)), ((), ())), preferred_element_type=F32
    )


def rows_of(refs):
    return jnp.concatenate([ref[...] for ref in refs], axis=0)


def early_kernel(
    own_ref, far_ref, whole_ref, gate_ref, up_ref, out_ref,
    weight_ref, token_ref, cot_ref, grad_ref, in_sems, out_sems,
):
    blocks, block, _ = weight_ref.shape
    mine, half, width = own_ref.shape[0], gate_ref.shape[1], token_ref.shape[1]
    rows = lambda k: pl.ds(k * block, block)
    loads = [
        pltpu.make_async_copy(whole_ref.at[rows(k)], weight_ref.at[k], in_sems.at[k])
        for k in range(blocks)
    ]
    stores = [
        pltpu.make_async_copy(grad_ref.at[k], out_ref.at[rows(k)], out_sems.at[k])
        for k in range(blocks)
    ]
    for load in loads:
        load.start()
    for at, ref in ((0, own_ref), (mine, far_ref)):
        token_ref[at : at + mine] = ref[:, width : 2 * width]
        cot_ref[at : at + mine] = ref[:, 2 * width :]
    both = 0.0
    for k in range(blocks):
        loads[k].wait()
        both += jnp.dot(token_ref[:, rows(k)], weight_ref[k], preferred_element_type=F32)
    gate, up = both[:, :half], both[:, half:]
    gate_ref[...] = gate
    up_ref[...] = up
    hidden = (gate / (1.0 + jnp.exp(-gate)) * up).astype(BF)
    for k in range(blocks):
        grad_ref[k] = lax.dot_general(
            cot_ref[:, rows(k)], hidden, (((0,), (0,)), ((), ())), preferred_element_type=F32
        ).astype(BF)
        stores[k].start()
    for store in stores:
        store.wait()


def early_part(tokens, whole):
    rows, width = 2 * tokens[0].shape[0], whole.shape[0]
    both, block = whole.shape[1], width // BLOCKS
    half = both // 2
    vmem, hbm = pl.BlockSpec(memory_space=pltpu.VMEM), pl.BlockSpec(memory_space=pltpu.HBM)
    return pl.pallas_call(
        early_kernel,
        in_specs=[vmem, vmem, hbm],
        out_specs=[vmem, vmem, hbm],
        out_shape=[
            jax.ShapeDtypeStruct((rows, half), F32),
            jax.ShapeDtypeStruct((rows, half), F32),
            pltpu.HBM((width, half), BF),
        ],
        scratch_shapes=[
            pltpu.VMEM((BLOCKS, block, both), BF),
            pltpu.VMEM((rows, width), BF),
            pltpu.VMEM((rows, width), BF),
            pltpu.VMEM((BLOCKS, block, half), BF),
            pltpu.SemaphoreType.DMA((BLOCKS,)),
            pltpu.SemaphoreType.DMA((BLOCKS,)),
        ],
        compiler_params=pltpu.CompilerParams(vmem_limit_bytes=16 << 20),
        cost_estimate=pl.CostEstimate(
            flops=6 * rows * width * half, transcendentals=rows * half, bytes_accessed=8 << 20
        ),
    )(*tokens, whole)


def rest_kernel(
    row_ref, own_in_ref, far_in_ref, cot_ref, cot_far_ref, weight_ref, gate_ref, up_ref, *others
):
    chunk_refs, (own_ref, other_ref) = others[:8], others[8:10]
    down_ref, sum_ref, grad_ref, hidden_ref, to_gate_ref, to_up_ref = others[10:]
    step = pl.program_id(0)
    half, lines = gate_ref.shape[1], down_ref.shape[0] // BLOCKS
    mine = own_ref.shape[1]

    @pl.when(step == 0)
    def _():
        sum_ref[...] = jnp.zeros_like(sum_ref)
        grad_ref[...] = jnp.zeros_like(grad_ref)
        for offset, chunk_ref in zip(OFFSETS, chunk_refs):
            at = (row_ref[0] + offset) & (len(OFFSETS) - 1)
            down_ref[:, pl.ds(at, 1)] = chunk_ref[...][:, None]

    @pl.when(step < BLOCKS)
    def _():
        down = down_ref[pl.ds(step * lines, lines)].reshape(-1, half)
        block = rows_of((own_in_ref, far_in_ref))
        sum_ref[...] += jnp.dot(block, weight_ref[...], preferred_element_type=F32)
        cot = rows_of((cot_ref, cot_far_ref))
        grad_ref[...] += jnp.dot(cot, down, preferred_element_type=F32)

    @pl.when(step == BLOCKS - 1)
    def _():
        gate, up = sum_ref[:, :half], sum_ref[:, half:]
        hidden_ref[...] = (gate / (1.0 + jnp.exp(-gate)) * up).astype(BF)
        gate, grad = gate_ref[...], grad_ref[...]
        sig = 1.0 / (1.0 + jnp.exp(-gate))
        to_gate_ref[...] = (grad * up_ref[...] * sig * (1.0 + gate * (1.0 - sig))).astype(BF)
        to_up_ref[...] = (grad * (gate * sig)).astype(BF)

    @pl.when(step >= BLOCKS)
    def _():
        down = down_ref[pl.ds((step - BLOCKS) * lines, lines)].reshape(-1, half)
        out = dot_nt(hidden_ref[...], down)
        back = dot_nt(to_gate_ref[...], weight_ref[:, :half])
        back += dot_nt(to_up_ref[...], weight_ref[:, half:])
        own_ref[0], own_ref[1] = out[:mine], back[:mine]
        other_ref[0], other_ref[1] = out[mine:].astype(BF), back[mine:].astype(BF)


def rest_part(tokens, whole, gate_early, up_early, chunks):
    mine, (width, both) = tokens[0].shape[0], whole.shape
    rows = 2 * mine
    block, half = width // BLOCKS, both // 2
    lines = chunks[0].shape[0]
    first = lambda k: jnp.minimum(k, BLOCKS - 1)
    then = lambda k: jnp.maximum(k - BLOCKS, 0)
    whole_of = lambda array: pl.BlockSpec(array.shape, lambda k: (0,) * array.ndim)
    out_block = pl.BlockSpec((2, rows // 2, block), lambda k: (0, 0, then(k)))
    return pl.pallas_call(
        rest_kernel,
        grid=(2 * BLOCKS,),
        in_specs=[
            pl.BlockSpec(memory_space=pltpu.SMEM),
            *[pl.BlockSpec((mine, block), lambda k: (0, first(k)))] * 2,
            *[pl.BlockSpec((mine, block), lambda k: (0, 2 * BLOCKS + first(k)))] * 2,
            pl.BlockSpec((block, both), lambda k: (k % BLOCKS, 0)),
            whole_of(gate_early),
            whole_of(up_early),
            *map(whole_of, chunks),
        ],
        out_specs=[out_block, out_block],
        out_shape=[
            jax.ShapeDtypeStruct((2, rows // 2, width), F32),
            jax.ShapeDtypeStruct((2, rows // 2, width), BF),
        ],
        scratch_shapes=[
            pltpu.VMEM((lines, len(chunks), *chunks[0].shape[1:]), BF),
            pltpu.VMEM((rows, both), F32),
            pltpu.VMEM((rows, half), F32),
            pltpu.VMEM((rows, half), BF),
            pltpu.VMEM((rows, half), BF),
            pltpu.VMEM((rows, half), BF),
        ],
        compiler_params=pltpu.CompilerParams(
            dimension_semantics=("arbitrary",), vmem_limit_bytes=16 << 20
        ),
        cost_estimate=pl.CostEstimate(
            flops=12 * rows * width * half, transcendentals=2 * rows * half, bytes_accessed=16 << 20
        ),
    )(
        lax.axis_index("y").astype(jnp.int32)[None],
        *tokens,
        *tokens,
        whole,
        gate_early,
        up_early,
        *chunks,
    )


def final_kernel(parts_ref, sum_ref, out_ref, load_ref, sems, *, factor):
    count, size = load_ref.shape[:2]
    loads = [
        pltpu.make_async_copy(parts_ref.at[pl.ds(k * size, size)], load_ref.at[k], sems.at[k])
        for k in range(count)
    ]
    for load in loads:
        load.start()
    total = 0.0
    for k, load in enumerate(loads):
        load.wait()
        total += jnp.sum(load_ref[k].astype(F32), axis=0)
    out_ref[...] = sum_ref[...] + total * factor


def final_part(parts, running, factor):
    vmem, count = pl.BlockSpec(memory_space=pltpu.VMEM), 8
    return pl.pallas_call(
        functools.partial(final_kernel, factor=factor),
        in_specs=[pl.BlockSpec(memory_space=pltpu.HBM), vmem],
        out_specs=vmem,
        out_shape=jax.ShapeDtypeStruct(running.shape, F32),
        scratch_shapes=[
            pltpu.VMEM((count, parts.shape[0] // count, *parts.shape[1:]), BF),
            pltpu.SemaphoreType.DMA((count,)),
        ],
        compiler_params=pltpu.CompilerParams(vmem_limit_bytes=6 << 20),
    )(parts, running)


def shards(later, early, cotangent, gate_w, up_w, down_w, down_grad_sum):
    rows, _ = later.shape
    fan = fanned(lax.axis_size("y"), gate_w, up_w)
    line = lax.all_to_all(fan, "y", 0, 0)
    line = line.reshape(-1, line.shape[-1])
    whole = lax.all_gather(line, "z", axis=0, tiled=True)
    whole = pltpu.with_memory_space_constraint(whole, pltpu.HBM)
    tokens = copies(1, later, early, cotangent)[0]
    tokens = collect_tokens(tokens)
    tokens = [pltpu.with_memory_space_constraint(t, pltpu.VMEM) for t in tokens]
    chunks = gather_down(down_w)

    gate_early, up_early, down_grad = early_part(tokens, whole)
    received = lax.all_to_all(down_grad.reshape(-1, *gate_w.shape), FS, 0, 0)

    own, other = rest_part(tokens, whole, gate_early, up_early, chunks)
    later_output, earlier_grad_input = give_rows(own, other, rows)

    factor = (rows * lax.axis_size(AXES)) ** (-0.5)
    return later_output, earlier_grad_input, final_part(received, down_grad_sum, factor)


def solution(mesh):
    split = Mesh(mesh.devices.reshape(8, 8, 4, 2), AXES)
    tokens, weights = P(AXES, None), P(FS, ("x", "c"))
    return jax.shard_map(
        shards,
        mesh=split,
        in_specs=(tokens,) * 3 + (weights,) * 4,
        out_specs=(tokens, tokens, weights),
        check_vma=False,
    )
```

```python
import jax
import jax.numpy as jnp
from jax import lax
from jax.experimental import pallas as pl
from jax.experimental.pallas import tpu as pltpu
from jax.sharding import Mesh
from jax.sharding import PartitionSpec as P


AXES = ("z", "y", "x", "c")
FS = ("z", "y")
STEPS = (0, 1, -1, 2)
BLOCKS = 4
OFFSETS = (0, -1, 1, -2, 2, -3, 3, 4)
BF, F32 = jnp.bfloat16, jnp.float32


def shift(value, axis, step):
    count = lax.axis_size(axis)
    if step == 0:
        return value
    return lax.ppermute(value, axis, [(i, (i + step) % count) for i in range(count)])


def copy_kernel(*refs):
    *ins, out_ref = refs
    at = 0
    for ref in ins:
        cols = ref.shape[1]
        out_ref[:, :, at : at + cols] = jnp.broadcast_to(ref[...], (out_ref.shape[0], *ref.shape))
        at += cols


def copies(count, *arrays):
    shape = (count, arrays[0].shape[0], sum(a.shape[1] for a in arrays))
    return pl.pallas_call(
        copy_kernel,
        out_shape=jax.ShapeDtypeStruct(shape, arrays[0].dtype),
        compiler_params=pltpu.CompilerParams(vmem_limit_bytes=8 << 20),
        cost_estimate=pl.CostEstimate(flops=1 << 20, transcendentals=0, bytes_accessed=1 << 20),
    )(*[pltpu.with_memory_space_constraint(a, pltpu.HBM) for a in arrays])


def fan_kernel(*refs):
    *ins, out_ref, side_ref, sems = refs
    at, loads = 0, []
    for ref in ins:
        cols = ref.shape[1]
        place = side_ref.at[:, pl.ds(at, cols)]
        loads.append(pltpu.make_async_copy(ref, place, sems.at[len(loads)]))
        at += cols
    stores = [
        pltpu.make_async_copy(side_ref, out_ref.at[k], sems.at[len(loads) + k])
        for k in range(out_ref.shape[0])
    ]
    for group in (loads, stores):
        for move in group:
            move.start()
        for move in group:
            move.wait()


def fanned(count, *arrays):
    side = (arrays[0].shape[0], sum(a.shape[1] for a in arrays))
    hbm = pl.BlockSpec(memory_space=pltpu.HBM)
    return pl.pallas_call(
        fan_kernel,
        in_specs=[hbm] * len(arrays),
        out_specs=hbm,
        out_shape=pltpu.HBM((count, *side), arrays[0].dtype),
        scratch_shapes=[
            pltpu.VMEM(side, arrays[0].dtype),
            pltpu.SemaphoreType.DMA((count + len(arrays),)),
        ],
        compiler_params=pltpu.CompilerParams(vmem_limit_bytes=4 << 20),
        cost_estimate=pl.CostEstimate(flops=1 << 20, transcendentals=0, bytes_accessed=1 << 20),
    )(*[pltpu.with_memory_space_constraint(a, pltpu.HBM) for a in arrays])


def stack_kernel(*refs):
    *ins, out_ref = refs
    for at, ref in enumerate(ins):
        rows = ref.shape[0]
        out_ref[at * rows : (at + 1) * rows] = ref[...]


def stacked(pieces):
    rows, cols = pieces[0].shape
    return pl.pallas_call(
        stack_kernel,
        out_shape=jax.ShapeDtypeStruct((len(pieces) * rows, cols), pieces[0].dtype),
        compiler_params=pltpu.CompilerParams(vmem_limit_bytes=8 << 20),
        cost_estimate=pl.CostEstimate(flops=1 << 20, transcendentals=0, bytes_accessed=1 << 20),
    )(*pieces)


def gather_down(down):
    fan = fanned(lax.axis_size("z"), down)
    line = lax.all_to_all(fan, "z", 0, 0)
    chunks, ahead, behind = [line], line, line
    for _ in range(1, 4):
        ahead, behind = shift(ahead, "y", 1), shift(behind, "y", -1)
        chunks += [ahead, behind]
    return [*chunks, shift(ahead, "y", 1)]


def collect_tokens(own):
    pieces = [shift(own, "x", step) for step in STEPS]
    line = stacked(pieces)
    other = shift(line, "c", 1)
    return line, other


def give_rows(own, other, rows):
    both = (own + shift(other, "c", 1).astype(F32)).astype(BF)
    total = 0.0
    for at, step in enumerate(STEPS):
        total += shift(both[:, at * rows : (at + 1) * rows], "x", -step).astype(F32)
    return total.astype(BF)


def dot_nt(leading, trailing):
    return lax.dot_general(
        leading, trailing, (((1,), (1,)), ((), ())), preferred_element_type=F32
    )


def rows_of(refs):
    return jnp.concatenate([ref[...] for ref in refs], axis=0)


def early_kernel(
    own_ref, far_ref, whole_ref, gate_ref, up_ref, out_ref,
    weight_ref, token_ref, cot_ref, grad_ref, in_sems, out_sems,
):
    blocks, block, _ = weight_ref.shape
    mine, half, width = own_ref.shape[0], gate_ref.shape[1], token_ref.shape[1]
    rows = lambda k: pl.ds(k * block, block)
    loads = [
        pltpu.make_async_copy(whole_ref.at[rows(k)], weight_ref.at[k], in_sems.at[k])
        for k in range(blocks)
    ]
    stores = [
        pltpu.make_async_copy(grad_ref.at[k], out_ref.at[rows(k)], out_sems.at[k])
        for k in range(blocks)
    ]
    for load in loads:
        load.start()
    for at, ref in ((0, own_ref), (mine, far_ref)):
        token_ref[at : at + mine] = ref[:, width : 2 * width]
        cot_ref[at : at + mine] = ref[:, 2 * width :]
    both = 0.0
    for k in range(blocks):
        loads[k].wait()
        both += jnp.dot(token_ref[:, rows(k)], weight_ref[k], preferred_element_type=F32)
    gate, up = both[:, :half], both[:, half:]
    gate_ref[...] = gate
    up_ref[...] = up
    hidden = (gate / (1.0 + jnp.exp(-gate)) * up).astype(BF)
    for k in range(blocks):
        grad_ref[k] = lax.dot_general(
            cot_ref[:, rows(k)], hidden, (((0,), (0,)), ((), ())), preferred_element_type=F32
        ).astype(BF)
        stores[k].start()
    for store in stores:
        store.wait()


def early_part(tokens, whole):
    rows, width = 2 * tokens[0].shape[0], whole.shape[0]
    both, block = whole.shape[1], width // BLOCKS
    half = both // 2
    vmem, hbm = pl.BlockSpec(memory_space=pltpu.VMEM), pl.BlockSpec(memory_space=pltpu.HBM)
    return pl.pallas_call(
        early_kernel,
        in_specs=[vmem, vmem, hbm],
        out_specs=[vmem, vmem, hbm],
        out_shape=[
            jax.ShapeDtypeStruct((rows, half), F32),
            jax.ShapeDtypeStruct((rows, half), F32),
            pltpu.HBM((width, half), BF),
        ],
        scratch_shapes=[
            pltpu.VMEM((BLOCKS, block, both), BF),
            pltpu.VMEM((rows, width), BF),
            pltpu.VMEM((rows, width), BF),
            pltpu.VMEM((BLOCKS, block, half), BF),
            pltpu.SemaphoreType.DMA((BLOCKS,)),
            pltpu.SemaphoreType.DMA((BLOCKS,)),
        ],
        compiler_params=pltpu.CompilerParams(vmem_limit_bytes=16 << 20),
        cost_estimate=pl.CostEstimate(
            flops=6 * rows * width * half, transcendentals=rows * half, bytes_accessed=8 << 20
        ),
    )(*tokens, whole)


def rest_kernel(
    row_ref, own_in_ref, far_in_ref, cot_ref, cot_far_ref, weight_ref, gate_ref, up_ref, *others
):
    chunk_refs, (own_ref, other_ref) = others[:8], others[8:10]
    down_ref, sum_ref, grad_ref, hidden_ref, to_gate_ref, to_up_ref = others[10:]
    step = pl.program_id(0)
    half, lines = gate_ref.shape[1], down_ref.shape[0] // BLOCKS
    mine = own_ref.shape[1]

    @pl.when(step == 0)
    def _():
        sum_ref[...] = jnp.zeros_like(sum_ref)
        grad_ref[...] = jnp.zeros_like(grad_ref)
        for offset, chunk_ref in zip(OFFSETS, chunk_refs):
            at = (row_ref[0] + offset) & (len(OFFSETS) - 1)
            down_ref[:, pl.ds(at, 1)] = chunk_ref[...][:, None]

    @pl.when(step < BLOCKS)
    def _():
        down = down_ref[pl.ds(step * lines, lines)].reshape(-1, half)
        block = rows_of((own_in_ref, far_in_ref))
        sum_ref[...] += jnp.dot(block, weight_ref[...], preferred_element_type=F32)
        cot = rows_of((cot_ref, cot_far_ref))
        grad_ref[...] += jnp.dot(cot, down, preferred_element_type=F32)

    @pl.when(step == BLOCKS - 1)
    def _():
        gate, up = sum_ref[:, :half], sum_ref[:, half:]
        hidden_ref[...] = (gate / (1.0 + jnp.exp(-gate)) * up).astype(BF)
        gate, grad = gate_ref[...], grad_ref[...]
        sig = 1.0 / (1.0 + jnp.exp(-gate))
        to_gate_ref[...] = (grad * up_ref[...] * sig * (1.0 + gate * (1.0 - sig))).astype(BF)
        to_up_ref[...] = (grad * (gate * sig)).astype(BF)

    @pl.when(step >= BLOCKS)
    def _():
        down = down_ref[pl.ds((step - BLOCKS) * lines, lines)].reshape(-1, half)
        out = dot_nt(hidden_ref[...], down)
        back = dot_nt(to_gate_ref[...], weight_ref[:, :half])
        back += dot_nt(to_up_ref[...], weight_ref[:, half:])
        own_ref[0], own_ref[1] = out[:mine], back[:mine]
        other_ref[0], other_ref[1] = out[mine:].astype(BF), back[mine:].astype(BF)


def rest_part(tokens, whole, gate_early, up_early, chunks):
    mine, (width, both) = tokens[0].shape[0], whole.shape
    rows = 2 * mine
    block, half = width // BLOCKS, both // 2
    lines = chunks[0].shape[0]
    first = lambda k: jnp.minimum(k, BLOCKS - 1)
    then = lambda k: jnp.maximum(k - BLOCKS, 0)
    whole_of = lambda array: pl.BlockSpec(array.shape, lambda k: (0,) * array.ndim)
    out_block = pl.BlockSpec((2, rows // 2, block), lambda k: (0, 0, then(k)))
    return pl.pallas_call(
        rest_kernel,
        grid=(2 * BLOCKS,),
        in_specs=[
            pl.BlockSpec(memory_space=pltpu.SMEM),
            *[pl.BlockSpec((mine, block), lambda k: (0, first(k)))] * 2,
            *[pl.BlockSpec((mine, block), lambda k: (0, 2 * BLOCKS + first(k)))] * 2,
            pl.BlockSpec((block, both), lambda k: (k % BLOCKS, 0)),
            whole_of(gate_early),
            whole_of(up_early),
            *map(whole_of, chunks),
        ],
        out_specs=[out_block, out_block],
        out_shape=[
            jax.ShapeDtypeStruct((2, rows // 2, width), F32),
            jax.ShapeDtypeStruct((2, rows // 2, width), BF),
        ],
        scratch_shapes=[
            pltpu.VMEM((lines, len(chunks), *chunks[0].shape[1:]), BF),
            pltpu.VMEM((rows, both), F32),
            pltpu.VMEM((rows, half), F32),
            pltpu.VMEM((rows, half), BF),
            pltpu.VMEM((rows, half), BF),
            pltpu.VMEM((rows, half), BF),
        ],
        compiler_params=pltpu.CompilerParams(
            dimension_semantics=("arbitrary",), vmem_limit_bytes=16 << 20
        ),
        cost_estimate=pl.CostEstimate(
            flops=12 * rows * width * half, transcendentals=2 * rows * half, bytes_accessed=16 << 20
        ),
    )(
        lax.axis_index("y").astype(jnp.int32)[None],
        *tokens,
        *tokens,
        whole,
        gate_early,
        up_early,
        *chunks,
    )


def shards(later, early, cotangent, gate_w, up_w, down_w, down_grad_sum):
    rows, _ = later.shape
    fan = fanned(lax.axis_size("y"), gate_w, up_w)
    line = lax.all_to_all(fan, "y", 0, 0)
    line = line.reshape(-1, line.shape[-1])
    whole = lax.all_gather(line, "z", axis=0, tiled=True)
    whole = pltpu.with_memory_space_constraint(whole, pltpu.HBM)
    tokens = copies(1, later, early, cotangent)[0]
    tokens = collect_tokens(tokens)
    tokens = [pltpu.with_memory_space_constraint(t, pltpu.VMEM) for t in tokens]
    chunks = gather_down(down_w)

    gate_early, up_early, down_grad = early_part(tokens, whole)
    received = lax.all_to_all(down_grad.reshape(-1, *gate_w.shape), FS, 0, 0)

    own, other = rest_part(tokens, whole, gate_early, up_early, chunks)
    later_output, earlier_grad_input = give_rows(own, other, rows)

    summed = jnp.sum(received.astype(F32), axis=0)
    factor = (rows * lax.axis_size(AXES)) ** (-0.5)
    return later_output, earlier_grad_input, down_grad_sum + summed * factor


def solution(mesh):
    split = Mesh(mesh.devices.reshape(8, 8, 4, 2), AXES)
    tokens, weights = P(AXES, None), P(FS, ("x", "c"))
    return jax.shard_map(
        shards,
        mesh=split,
        in_specs=(tokens,) * 3 + (weights,) * 4,
        out_specs=(tokens, tokens, weights),
        check_vma=False,
    )
```
